512 devices in a mesh: kv: 32 (over z, core), tp: 16 (over y, x).
Axes of the slice: x: 4, y: 4, z: 16, core: 2. Of those that a mesh axis runs over, the one named last changes fastest.
Arguments:
- tokens: bfloat16 [256, 4096], P(None, ('kv', 'tp')), may hold values from -3 to 3
- lengths: int32 [64], replicated, may hold values from 1 to 4, 128 in all
- states: float32 [64, 16, 128, 128], P('kv', 'tp'), may hold values from -3 to 3
- gain_pre: float32 [4096], P('kv'), may hold values from 0.1 to 1.9
- pre_gate: bfloat16 [4096, 11264], P('kv', 'tp'), may hold values from -0.09375 to 0.09375
- pre_up: bfloat16 [4096, 11264], P('kv', 'tp'), may hold values from -0.09375 to 0.09375
- pre_down: bfloat16 [11264, 4096], P('tp', 'kv'), may hold values from -1 to 1
- gain_mix: float32 [4096], P('kv'), may hold values from 0.1 to 1.9
- query_weight: bfloat16 [4096, 2048], P('kv', 'tp'), may hold values from -0.09375 to 0.09375
- forget_weight: bfloat16 [4096, 2048], P('kv', 'tp'), may hold values from -0.09375 to 0.09375
- input_weight: bfloat16 [4096, 2048], P('kv', 'tp'), may hold values from -0.09375 to 0.09375
- outgate_weight: bfloat16 [4096, 2048], P('kv', 'tp'), may hold values from -0.09375 to 0.09375
- forget_floor: float32 [2048], P('tp'), may hold values from 0 to 0.9
- head_gain: float32 [128], replicated, may hold values from 0.1 to 1.9
- mix_weight: bfloat16 [2048, 4096], P('tp', 'kv'), may hold values from -1 to 1
- gain_post: float32 [4096], P('kv'), may hold values from 0.1 to 1.9
- post_gate: bfloat16 [4096, 11264], P('kv', 'tp'), may hold values from -0.09375 to 0.09375
- post_up: bfloat16 [4096, 11264], P('kv', 'tp'), may hold values from -0.09375 to 0.09375
- post_down: bfloat16 [11264, 4096], P('tp', 'kv'), may hold values from -0.0546875 to 0.0546875
Outputs:
- out_tokens: bfloat16 [256, 4096], P(None, ('kv', 'tp'))
- new_states: float32 [64, 16, 128, 128], P('kv', 'tp')
The draws below stay inside these ranges and needn't reach their ends.
Inputs may be any that keep to these rules, and one draw needn't show every extreme that they name: `lengths`: each of the 64 sequences has 1 to 4 new tokens, 128 in all, and at least one has exactly 4.
All inputs are finite; a program needn't handle non-finite values.
Results may differ from the reference program's by a relative error of at most 0.011.
Values may be sent and summed in bfloat16 or wider, within the bound.
No kernel may reach another device: no remote copies, remote signals or barrier semaphores. Data moves between devices by JAX's collectives and lax.ppermute only.
A program may use at most 64 MiB of HBM per device.

```python
import math
import jax
import jax.numpy as jnp
import numpy as np
from jax import lax

D = 4096
FF = 11264
HEADS = 16
DK = 128
W = 4
BATCH = 64
ROWS = 256
HW = 2048


def draw_tokens(key, part):
    noise_key = jax.random.fold_in(key, 11)
    phase_key = jax.random.fold_in(key, 12)
    shrink_key = jax.random.fold_in(key, 14)
    columns = jnp.arange(D, dtype=jnp.float32) / D
    phase_shift = jax.random.uniform(phase_key, (), jnp.float32, 0.0, 6.283)
    profile = jnp.exp(1.2 * jnp.cos(6.283 * columns + phase_shift))
    shrink = jnp.exp(jax.random.uniform(shrink_key, (ROWS, 1), jnp.float32, -4.0, -2.0))
    samples = jnp.clip(jax.random.normal(noise_key, (ROWS, D), jnp.float32), -6.0, 6.0)
    return (samples * profile[None, :] * shrink).astype(jnp.bfloat16)


def column_levels(key, stream):
    level_key = jax.random.fold_in(key, stream)
    groups = D // 64
    exponents = jax.random.uniform(level_key, (groups,), jnp.float32, -1.5, 1.5)
    return jnp.repeat(jnp.exp(exponents), 64)


def draw_pre_down(key, part):
    noise_key = jax.random.fold_in(key, 21)
    samples = jnp.clip(jax.random.normal(noise_key, (FF, D), jnp.float32), -4.0, 4.0)
    levels = column_levels(key, 22)
    return (samples * levels[None, :] / jnp.sqrt(jnp.float32(FF))).astype(jnp.bfloat16)


def draw_mix_weight(key, part):
    noise_key = jax.random.fold_in(key, 31)
    samples = jnp.clip(jax.random.normal(noise_key, (HW, D), jnp.float32), -4.0, 4.0)
    levels = column_levels(key, 32)
    return (samples * levels[None, :] / jnp.sqrt(jnp.float32(HW))).astype(jnp.bfloat16)


def steps_of(stream_key, extent, shards, low, largest):
    level, own = 1.0, jax.random.fold_in(stream_key, 6)
    for axis_at, parts in shards:
        steps = jnp.exp(jax.random.uniform(jax.random.fold_in(own, axis_at), (parts,), jnp.float32, low / len(shards), largest / len(shards)))
        level = level * jnp.repeat(steps, extent[axis_at] // parts).reshape([-1 if axis == axis_at else 1 for axis in range(len(extent))])
    return level


def length_profile(count, total, reach, skew):
    portions = [(1 << 20) // math.isqrt(rank ** skew) + 1 for rank in range(2, count + 1)]
    surplus, given = total - reach - (count - 1), [1] * (count - 1)
    while surplus > 0:
        movable = [i for i in range(count - 1) if given[i] < reach]
        whole, budget = sum([portions[i] for i in movable]), surplus
        for i in movable:
            more = min(reach - given[i], max(1, budget * portions[i] // whole), surplus)
            given[i] = given[i] + more
            surplus = surplus - more
    return np.array([reach] + given)


def uneven(key, amount, total, reach, skew):
    if amount == 2:
        one = jax.random.randint(key, (), max(1, total - reach), min(reach, total - 1) + 1)
        return jnp.stack([one, total - one])
    sizes = jnp.asarray(length_profile(amount, total, reach, skew), jnp.int32)
    pairs = (amount - 1) // 2
    donor, receiver = sizes[1:1 + 2 * pairs:2], sizes[2:2 + 2 * pairs:2]
    room = jnp.minimum(donor - 1, reach - receiver)
    moved = jax.random.randint(jax.random.fold_in(key, 1), (pairs,), 0, 1 << 20) % (room + 1)
    sizes = sizes.at[1:1 + 2 * pairs:2].set(donor - moved).at[2:2 + 2 * pairs:2].set(receiver + moved)
    return sizes[jax.random.permutation(jax.random.fold_in(key, 2), amount)]


def noise(stream_key, dims, scale, reach, cuts=(), held_as=jnp.bfloat16):
    factor_of = steps_of(stream_key, dims, cuts, -0.22, 0.18) if cuts else 1.0
    drawn = jax.random.normal(stream_key, dims, jnp.float32) * scale * factor_of
    return jnp.minimum(jnp.maximum(drawn, -reach), reach).astype(held_as)


def setup_inputs(seed: int = 0) -> dict:
    keys = jax.random.split(jax.random.key(seed), 20)
    return {
        "tokens": draw_tokens(jax.random.fold_in(keys[19], 71), 0),
        "lengths": uneven(keys[1], BATCH, 2 * BATCH, W, 2).astype(jnp.int32),
        "states": noise(keys[2], (BATCH, HEADS, DK, DK), 0.5, 3.0, ((0, 32), (1, 16)), jnp.float32),
        "gain_pre": jnp.clip(1.0 + 0.18 * jax.random.normal(keys[3], (D,), jnp.float32), 0.1, 1.9),
        "pre_gate": noise(keys[4], (D, FF), D ** -0.5, 0.09375, ((0, 32), (1, 16))),
        "pre_up": noise(keys[5], (D, FF), D ** -0.5, 0.09375, ((0, 32), (1, 16))),
        "pre_down": draw_pre_down(jax.random.fold_in(keys[19], 71), 0),
        "gain_mix": jnp.clip(1.0 + 0.18 * jax.random.normal(keys[7], (D,), jnp.float32), 0.1, 1.9),
        "query_weight": noise(keys[8], (D, HW), D ** -0.5, 0.09375, ((0, 32), (1, 16))),
        "forget_weight": noise(keys[9], (D, HW), D ** -0.5, 0.09375, ((0, 32), (1, 16))),
        "input_weight": noise(keys[10], (D, HW), D ** -0.5, 0.09375, ((0, 32), (1, 16))),
        "outgate_weight": noise(keys[11], (D, HW), D ** -0.5, 0.09375, ((0, 32), (1, 16))),
        "forget_floor": jnp.clip(0.9 * jax.random.uniform(keys[12], (HW,), jnp.float32) ** steps_of(keys[12], (HW,), ((0, 16),), -0.2, 0.2), 0.0, 0.9),
        "head_gain": jnp.clip(1.0 + 0.18 * jax.random.normal(keys[13], (DK,), jnp.float32), 0.1, 1.9),
        "mix_weight": draw_mix_weight(jax.random.fold_in(keys[19], 71), 0),
        "gain_post": jnp.clip(1.0 + 0.18 * jax.random.normal(keys[15], (D,), jnp.float32), 0.1, 1.9),
        "post_gate": noise(keys[16], (D, FF), D ** -0.5, 0.09375, ((0, 32), (1, 16))),
        "post_up": noise(keys[17], (D, FF), D ** -0.5, 0.09375, ((0, 32), (1, 16))),
        "post_down": noise(keys[18], (FF, D), FF ** -0.5, 0.0546875, ((0, 16), (1, 32))),
    }


EPSILON = 1e-06

def normalize(values, gain):
    floats = values.astype(jnp.float32)
    meansq = lax.optimization_barrier(jnp.mean(floats * floats, axis=1, keepdims=True))
    return (floats * lax.rsqrt(meansq + EPSILON) * gain).astype(jnp.bfloat16)

def half_mixer(values, gain, gate_weight, up_weight, down_weight):
    normed = normalize(values, gain)
    gate_part = jnp.dot(normed, gate_weight, preferred_element_type=jnp.float32)
    up_part = jnp.dot(normed, up_weight, preferred_element_type=jnp.float32)
    hidden = (jax.nn.silu(gate_part) * up_part).astype(jnp.bfloat16)
    return jnp.dot(hidden, down_weight, preferred_element_type=jnp.float32)

def reference(tokens, lengths, states, gain_pre, pre_gate, pre_up, pre_down, gain_mix, query_weight, forget_weight, input_weight, outgate_weight, forget_floor, head_gain, mix_weight, gain_post, post_gate, post_up, post_down):
    resid_one = (tokens.astype(jnp.float32) + 0.5 * half_mixer(tokens, gain_pre, pre_gate, pre_up, pre_down)).astype(jnp.bfloat16)
    normed = normalize(resid_one, gain_mix)
    shape_four = (BATCH, W, HEADS, DK)
    queries = jax.nn.silu(jnp.dot(normed, query_weight, preferred_element_type=jnp.float32)).reshape(shape_four)
    forget_raw = jnp.dot(normed, forget_weight, preferred_element_type=jnp.float32).reshape(shape_four)
    fresh_values = jnp.dot(normed, input_weight, preferred_element_type=jnp.float32).reshape(shape_four)
    gating = jnp.dot(normed, outgate_weight, preferred_element_type=jnp.float32).reshape(shape_four)
    live_mask = jnp.arange(W, dtype=jnp.int32)[None, :] < lengths[:, None]
    live_four = live_mask[:, :, None, None]
    floors = forget_floor.reshape(HEADS, DK)
    forgets = jnp.where(live_four, floors + (1.0 - floors) * jax.nn.sigmoid(forget_raw), jnp.float32(1.0))
    write_rate = 1.0 - forgets
    carried = states
    readings = []
    for offset in range(W):
        carried = forgets[:, offset, :, :, None] * carried + write_rate[:, offset, :, :, None] * fresh_values[:, offset, :, None, :]
        readings.append(jnp.einsum('bhk,bhkv->bhv', queries[:, offset], carried, precision=lax.Precision.HIGHEST))
    read_out = jnp.stack(readings, axis=1)
    meansq = lax.optimization_barrier(jnp.mean(read_out * read_out, axis=3, keepdims=True))
    head_out = (read_out * lax.rsqrt(meansq + EPSILON) * head_gain * jax.nn.silu(gating) * live_four.astype(jnp.float32)).astype(jnp.bfloat16).reshape(BATCH * W, HEADS * DK)
    mixed = jnp.dot(head_out, mix_weight, preferred_element_type=jnp.float32)
    resid_two = (resid_one.astype(jnp.float32) + mixed).astype(jnp.bfloat16)
    live_rows = live_mask.reshape(BATCH * W, 1).astype(jnp.float32)
    outcome = ((resid_two.astype(jnp.float32) + 0.5 * half_mixer(resid_two, gain_post, post_gate, post_up, post_down)) * live_rows).astype(jnp.bfloat16)
    return (outcome, carried)
```

```python
import jax
import jax.numpy as jnp
from jax import lax
from jax.sharding import Mesh
from jax.sharding import PartitionSpec as P

D = 4096
DK = 128
W = 4
EPSILON = 1e-06
LANES = 128

f32 = jnp.float32
bf16 = jnp.bfloat16


def exchanged(value, axis):
    return lax.all_to_all(value, axis, split_axis=0, concat_axis=0, tiled=True)


def sent_to_all(value, axis):
    return exchanged(jnp.broadcast_to(value, (lax.axis_size(axis), *value.shape)), axis)


def matmul(a, b):
    return jnp.dot(a, b, preferred_element_type=f32)


def split_three(values):
    high = lax.reduce_precision(values, 8, 7)
    rest = values - high
    mid = lax.reduce_precision(rest, 8, 7)
    return high, mid, rest - mid


def lane_padded(value, width):
    return jnp.pad(value, ((0, 0), (0, width - value.shape[1])))


def squares_of(rows):
    wide = rows.astype(f32)
    total = jnp.sum(wide * wide, axis=1, keepdims=True)
    high = lax.reduce_precision(total, 8, 7)
    return high, total - high


def slot_targets(lengths, slot_count):
    seq_count = lengths.shape[0]
    seqs = jnp.arange(seq_count, dtype=jnp.int32)
    slots = jnp.arange(slot_count, dtype=jnp.int32)
    seq_of = slots // W
    within = slots % W
    before = jnp.sum(jnp.where(seqs[None, :] < seq_of[:, None], lengths[None, :], 0), axis=1)
    own = jnp.sum(jnp.where(seqs[None, :] == seq_of[:, None], lengths[None, :], 0), axis=1)
    return jnp.where(within < own, before + within, -1)


def local(
    tokens,
    lengths,
    states,
    gain_pre,
    pre_gate,
    pre_up,
    pre_down,
    gain_mix,
    query_weight,
    forget_weight,
    input_weight,
    outgate_weight,
    forget_floor,
    head_gain,
    mix_weight,
    gain_post,
    post_gate,
    post_up,
    post_down,
):
    core = lax.axis_index("c")
    z_count = lax.axis_size("z")
    tp_count = lax.axis_size("tp")
    slot_count = tokens.shape[0]
    packed = slot_count // 2
    half = packed // 2
    per_z = half // z_count
    own_cols = gain_pre.shape[0]
    hidden = pre_gate.shape[1]
    wide = -(-hidden // LANES) * LANES
    head_cols = query_weight.shape[1]
    seq_local, heads_local = states.shape[:2]

    downs = jnp.concatenate([pre_down, post_down], axis=0)
    down_blocks = 2 * hidden // own_cols
    gain_rows = jnp.stack(
        [piece for gain in (gain_pre, gain_mix, gain_post) for piece in split_three(gain)]
    ).astype(bf16)
    gain_block = jnp.pad(gain_rows, ((0, own_cols - gain_rows.shape[0]), (0, 0)))
    mine = jnp.concatenate(
        [
            lane_padded(pre_gate, wide),
            lane_padded(pre_up, wide),
            lane_padded(post_gate, wide),
            lane_padded(post_up, wide),
            query_weight,
            forget_weight,
            input_weight,
            outgate_weight,
            mix_weight,
            gain_block,
        ]
        + [downs[i * own_cols : (i + 1) * own_cols] for i in range(down_blocks)],
        axis=1,
    )
    theirs = lax.ppermute(mine, "c", [(0, 1), (1, 0)])

    def unpacked(bundle):
        at = 4 * wide
        both_ff = (bundle[:, : 2 * wide], bundle[:, 2 * wide : at])
        heads = bundle[:, at : at + 4 * head_cols]
        at += 4 * head_cols
        mix = bundle[:, at : at + own_cols]
        at += own_cols
        gains = bundle[:9, at : at + own_cols].astype(f32)
        gains = [gains[3 * i] + gains[3 * i + 1] + gains[3 * i + 2] for i in range(3)]
        at += own_cols
        down = jnp.concatenate(
            [bundle[:, at + i * own_cols : at + (i + 1) * own_cols] for i in range(down_blocks)],
            axis=0,
        )
        return both_ff, heads, mix, gains, (down[:hidden], down[hidden:])

    ff_mine, heads_mine, mix_mine, _, _ = unpacked(mine)
    gains_mine = (gain_pre, gain_mix, gain_post)
    down_mine = (pre_down, post_down)
    ff_other, heads_other, mix_other, gains_other, down_other = unpacked(theirs)

    def both_gains(i):
        return jnp.concatenate([gains_mine[i], gains_other[i]])[None, :]

    targets = slot_targets(lengths, slot_count)
    rows = jnp.arange(packed, dtype=jnp.int32)
    table = rows[:, None] == targets[None, :]
    table_half = table.astype(bf16)

    entry = lax.dot_general(
        tokens, table_half, (((0,), (1,)), ((), ())), preferred_element_type=f32
    ).astype(bf16)
    pieces = jnp.stack([entry[:, :half], entry[:, half:]])
    pieces = jnp.broadcast_to(pieces[:, None], (2, tp_count, *pieces.shape[1:]))
    gathered = exchanged(pieces.reshape(2 * tp_count, *pieces.shape[2:]), ("c", "tp"))
    gathered = gathered.reshape(2, own_cols, half)
    gathered = jnp.where(core == 0, gathered, gathered[::-1])
    resid = gathered.reshape(2 * own_cols, half).T

    def ff_hidden(resid, which):
        scaled = (resid.astype(f32) * both_gains(0 if which == 0 else 2)).astype(bf16)
        product = matmul(scaled[:, :own_cols], ff_mine[which]) + matmul(
            scaled[:, own_cols:], ff_other[which]
        )
        high, low = squares_of(resid)
        lanes = jnp.arange(2 * wide, dtype=jnp.int32)[None, :]
        product = jnp.where(lanes == hidden, high, jnp.where(lanes == hidden + 1, low, product))
        sent = product.astype(bf16).reshape(z_count, per_z, 2 * wide)
        owned = jnp.sum(exchanged(sent, "z").astype(f32), axis=0)
        total = owned[:, hidden : hidden + 1] + owned[:, hidden + 1 : hidden + 2]
        scale = lax.rsqrt(total / D + EPSILON)
        gate = owned[:, :hidden] * scale
        up = owned[:, wide : wide + hidden] * scale
        act = (jax.nn.silu(gate) * up).astype(bf16)
        return sent_to_all(act, "z").reshape(half, hidden)

    def tp_summed(partial):
        return jnp.sum(sent_to_all(partial.astype(bf16), "tp").astype(f32), axis=0)

    act = ff_hidden(resid, 0)
    partial = jnp.concatenate([matmul(act, down_mine[0]), matmul(act, down_other[0])], axis=1)
    resid_one = (resid.astype(f32) + 0.5 * tp_summed(partial)).astype(bf16)

    turned = jnp.concatenate([resid_one[:, own_cols:], resid_one[:, :own_cols]], axis=1)
    all_rows = jnp.concatenate([resid_one, lax.ppermute(turned, "c", [(0, 1), (1, 0)])], axis=0)
    row_ids = jnp.where(core == 0, rows, (rows + half) % packed)
    by_owner = targets.reshape(z_count, 2, seq_local * W)
    own_targets = jnp.where(core == 0, by_owner[:, 0], by_owner[:, 1]).reshape(packed)
    spread = (own_targets[:, None] == row_ids[None, :]).astype(bf16)
    slot_rows = matmul(spread, all_rows).astype(bf16)
    scaled = (slot_rows.astype(f32) * both_gains(1)).astype(bf16)
    product = matmul(scaled[:, :own_cols], heads_mine) + matmul(scaled[:, own_cols:], heads_other)
    high, low = squares_of(slot_rows)
    lanes = jnp.arange(LANES, dtype=jnp.int32)[None, :]
    stats = jnp.where(lanes == 0, high, jnp.where(lanes == 1, low, 0.0))
    sent = jnp.concatenate([product, stats], axis=1).astype(bf16)
    sent = sent.reshape(z_count, seq_local * W, 4 * head_cols + LANES)
    owned = jnp.sum(exchanged(sent, "z").astype(f32), axis=0)
    at = 4 * head_cols
    total = owned[:, at : at + 1] + owned[:, at + 1 : at + 2]
    owned = owned[:, :at] * lax.rsqrt(total / D + EPSILON)

    shape_four = (seq_local, W, heads_local, DK)
    queries = jax.nn.silu(owned[:, :head_cols]).reshape(shape_four)
    forget_raw = owned[:, head_cols : 2 * head_cols].reshape(shape_four)
    fresh_values = owned[:, 2 * head_cols : 3 * head_cols].reshape(shape_four)
    gating = owned[:, 3 * head_cols :].reshape(shape_four)
    first_seq = (lax.axis_index("z") * 2 + core) * seq_local
    local_lengths = lax.dynamic_slice_in_dim(lengths, first_seq, seq_local)
    live_mask = jnp.arange(W, dtype=jnp.int32)[None, :] < local_lengths[:, None]
    live_four = live_mask[:, :, None, None]
    floors = forget_floor.reshape(heads_local, DK)
    forgets = jnp.where(
        live_four, floors + (1.0 - floors) * jax.nn.sigmoid(forget_raw), jnp.float32(1.0)
    )
    write_rate = 1.0 - forgets
    carried = states
    readings = []
    for offset in range(W):
        carried = (
            forgets[:, offset, :, :, None] * carried
            + write_rate[:, offset, :, :, None] * fresh_values[:, offset, :, None, :]
        )
        readings.append(jnp.sum(queries[:, offset, :, :, None] * carried, axis=2))
    read_out = jnp.stack(readings, axis=1)
    meansq = jnp.mean(read_out * read_out, axis=3, keepdims=True)
    head_out = (
        (
            read_out
            * lax.rsqrt(meansq + EPSILON)
            * head_gain
            * jax.nn.silu(gating)
            * live_four.astype(f32)
        )
        .astype(bf16)
        .reshape(seq_local * W, heads_local * DK)
    )
    all_heads = sent_to_all(head_out, ("z", "c")).reshape(slot_count, heads_local * DK)
    my_table = jnp.where(core == 0, table_half[:half], table_half[half:])
    head_rows = matmul(my_table, all_heads).astype(bf16)
    partial = jnp.concatenate([matmul(head_rows, mix_mine), matmul(head_rows, mix_other)], axis=1)
    resid_two = (resid_one.astype(f32) + tp_summed(partial)).astype(bf16)

    act = ff_hidden(resid_two, 1)
    contract = (((0,), (1,)), ((), ()))
    finish = jnp.stack(
        [
            lax.dot_general(down, act, contract, preferred_element_type=f32)
            for down in (down_mine[1], down_other[1])
        ]
    )
    first = (lax.axis_index("tp") == 0).astype(f32)
    residual = resid_two.astype(f32).T.reshape(2, own_cols, half)
    finish = 0.5 * finish + first * residual
    finish = jnp.where(core == 0, finish, finish[::-1])
    finish = finish.reshape(2 * tp_count, own_cols // tp_count, half)
    finished = jnp.sum(exchanged(finish, ("c", "tp")).reshape(2, tp_count, -1, half), axis=1)
    finished = jnp.concatenate([finished[0], finished[1]], axis=1).astype(bf16)
    outcome = lax.dot_general(
        table_half, finished, (((0,), (1,)), ((), ())), preferred_element_type=f32
    ).astype(bf16)
    return (outcome, carried)


def solution(mesh):
    kv = mesh.shape["kv"]
    tp = mesh.shape["tp"]
    cut = Mesh(mesh.devices.reshape(kv // 2, 2, tp), ("z", "c", "tp"))
    kv_axes = ("z", "c")
    placed = (
        P(None, ("z", "c", "tp")),
        P(),
        P(kv_axes, "tp", None, None),
        P(kv_axes),
        P(kv_axes, "tp"),
        P(kv_axes, "tp"),
        P("tp", kv_axes),
        P(kv_axes),
        P(kv_axes, "tp"),
        P(kv_axes, "tp"),
        P(kv_axes, "tp"),
        P(kv_axes, "tp"),
        P("tp"),
        P(),
        P("tp", kv_axes),
        P(kv_axes),
        P(kv_axes, "tp"),
        P(kv_axes, "tp"),
        P("tp", kv_axes),
    )
    return jax.shard_map(
        local,
        mesh=cut,
        in_specs=placed,
        out_specs=(P(None, ("z", "c", "tp")), P(kv_axes, "tp", None, None)),
        check_vma=False,
    )
```

```python
import jax
import jax.numpy as jnp
from jax import lax
from jax.experimental import pallas as pl
from jax.experimental.pallas import tpu as pltpu
from jax.sharding import Mesh
from jax.sharding import PartitionSpec as P

D = 4096
DK = 128
W = 4
EPSILON = 1e-06
LANES = 128
GAIN_ROWS = 16

f32 = jnp.float32
bf16 = jnp.bfloat16
barrier = lax.optimization_barrier


def matmul(a, b):
    return jnp.dot(a, b, preferred_element_type=f32)


def matmul_t(a, b):
    return lax.dot_general(a, b, (((1,), (1,)), ((), ())), preferred_element_type=f32)


def pack_kernel(*refs):
    weights, gains, out, sems = refs[:-5], refs[-5:-2], refs[-2], refs[-1]
    copies = []
    at = 0
    for i, ref in enumerate(weights):
        count = ref.shape[0]
        copies.append(pltpu.make_async_copy(ref, out.at[pl.ds(at, count)], sems.at[i]))
        copies[-1].start()
        at += count
    pieces = []
    for ref in gains:
        value = ref[...]
        high = value.astype(bf16).astype(f32)
        rest = value - high
        mid = rest.astype(bf16).astype(f32)
        pieces += [high, mid, rest - mid]
    pieces.append(jnp.zeros((GAIN_ROWS - len(pieces), LANES), f32))
    out[at:, :] = jnp.concatenate(pieces, axis=0).astype(bf16)
    for copy in copies:
        copy.wait()


def packed_weights(weights, gains):
    rows = sum(w.shape[0] for w in weights) + GAIN_ROWS
    return pl.pallas_call(
        pack_kernel,
        in_specs=[pl.BlockSpec(memory_space=pl.ANY)] * len(weights)
        + [pl.BlockSpec(memory_space=pltpu.VMEM)] * len(gains),
        out_specs=pl.BlockSpec(memory_space=pltpu.VMEM),
        out_shape=jax.ShapeDtypeStruct((rows, weights[0].shape[1]), bf16),
        scratch_shapes=[pltpu.SemaphoreType.DMA((len(weights),))],
    )(*weights, *[gain[None, :] for gain in gains])


def squares_of(rows, width):
    wide = rows.astype(f32)
    total = jnp.sum(wide * wide, axis=1, keepdims=True)
    high = lax.reduce_precision(total, 8, 7)
    lanes = lax.broadcasted_iota(jnp.int32, (1, width), 1)
    return jnp.where(lanes == 0, high, jnp.where(lanes == 1, total - high, 0.0))


def slot_targets(lengths, slot_count):
    seq_count = lengths.shape[0]
    seqs = jnp.arange(seq_count, dtype=jnp.int32)
    slots = jnp.arange(slot_count, dtype=jnp.int32)
    seq_of = slots // W
    within = slots % W
    before = jnp.sum(jnp.where(seqs[None, :] < seq_of[:, None], lengths[None, :], 0), axis=1)
    own = jnp.sum(jnp.where(seqs[None, :] == seq_of[:, None], lengths[None, :], 0), axis=1)
    return jnp.where(within < own, before + within, -1)


def products(rows, gain, exact, own, other, product):
    cols = rows.shape[1] // 2
    wide = rows.astype(f32) * gain
    parts = [wide.astype(bf16)]
    if exact:
        parts.append((wide - lax.reduce_precision(wide, 8, 7)).astype(bf16))
    return [
        sum(product(p[:, :cols], a) + product(p[:, cols:], b) for p in parts)
        for a, b in zip(own, other, strict=True)
    ]


def local(
    tokens,
    lengths,
    states,
    gain_pre,
    pre_gate,
    pre_up,
    pre_down,
    gain_mix,
    query_weight,
    forget_weight,
    input_weight,
    outgate_weight,
    forget_floor,
    head_gain,
    mix_weight,
    gain_post,
    post_gate,
    post_up,
    post_down,
):
    core = lax.axis_index("c")
    z_count = lax.axis_size("z")
    tp_count = lax.axis_size("tp")
    slot_count = tokens.shape[0]
    packed = slot_count // 2
    half = packed // 2
    per_z = half // z_count
    own_cols = gain_pre.shape[0]
    hidden = pre_gate.shape[1]
    wide = -(-hidden // LANES) * LANES
    head_cols = query_weight.shape[1]
    seq_local, heads_local = states.shape[:2]
    swap = [(0, 1), (1, 0)]

    side = {}

    def exchanged(value, axis):
        value, tied = barrier((value, dict(side)))
        value = lax.all_to_all(value, axis, split_axis=0, concat_axis=0, tiled=True)
        value, tied = barrier((value, tied))
        side.update(tied)
        return value

    def sent_to_all(value, axis):
        return exchanged(jnp.broadcast_to(value, (lax.axis_size(axis), *value.shape)), axis)

    ff_names = ("pre_gate", "pre_up", "post_gate", "post_up")
    head_names = ("query", "forget", "input", "outgate")
    names = (*ff_names, *head_names, "mix", "pre_down", "post_down")
    mine = (pre_gate.T, pre_up.T, post_gate.T, post_up.T)
    mine += (query_weight, forget_weight, input_weight, outgate_weight)
    mine += (mix_weight, pre_down, post_down)
    gains = (gain_pre, gain_mix, gain_post)
    bundle = lax.ppermute(packed_weights(mine, gains), "c", swap)

    targets = slot_targets(lengths, slot_count)
    rows = jnp.arange(packed, dtype=jnp.int32)
    table = (rows[:, None] == targets[None, :]).astype(bf16)
    row_ids = jnp.where(core == 0, rows, (rows + half) % packed)
    by_owner = targets.reshape(z_count, 2, seq_local * W)
    own_targets = jnp.where(core == 0, by_owner[:, 0], by_owner[:, 1]).reshape(packed)
    first_seq = (lax.axis_index("z") * 2 + core) * seq_local
    local_lengths = lax.dynamic_slice_in_dim(lengths, first_seq, seq_local)
    live = jnp.arange(W, dtype=jnp.int32)[None, :] < local_lengths[:, None]
    side["table"] = table
    side["my_table"] = jnp.where(core == 0, table[:half], table[half:])
    side["spread"] = (own_targets[:, None] == row_ids[None, :]).astype(bf16)
    side["live"] = live[:, :, None, None].astype(f32)
    side["floors"] = forget_floor.reshape(heads_local, DK)
    side["rises"] = 1.0 - side["floors"]

    entry = lax.dot_general(
        tokens, table, (((0,), (1,)), ((), ())), preferred_element_type=f32
    ).astype(bf16)
    pieces = jnp.stack([entry[:, :half], entry[:, half:]])
    pieces = jnp.broadcast_to(pieces[:, None], (2, tp_count, *pieces.shape[1:]))
    gathered = exchanged(pieces.reshape(2 * tp_count, *pieces.shape[2:]), ("c", "tp"))
    gathered = gathered.reshape(2, own_cols, half)
    gathered = jnp.where(core == 0, gathered, gathered[::-1])
    side["resid"] = gathered.reshape(2 * own_cols, half).T

    at = 0
    for name, weight in zip(names, mine, strict=True):
        side[name] = (weight, bundle[at : at + weight.shape[0]])
        at += weight.shape[0]
    parts = bundle[at : at + 3 * len(gains)].astype(f32)
    for i, gain in enumerate(gains):
        other = jnp.sum(parts[3 * i : 3 * i + 3], axis=0)
        side[f"gain{i}"] = jnp.concatenate([gain, other])[None, :]

    def ff_hidden(gain, names, exact):
        resid = side["resid"]
        own, other = zip(*[side[name] for name in names], strict=True)
        gate, up = products(resid, side[gain], exact, own, other, matmul_t)
        blank = jnp.zeros((half, wide - hidden), f32)
        sent = jnp.concatenate([gate, squares_of(resid, wide - hidden), up, blank], axis=1)
        sent = sent.astype(bf16).reshape(z_count, per_z, 2 * wide)
        owned = jnp.sum(exchanged(sent, "z").astype(f32), axis=0)
        total = owned[:, hidden : hidden + 1] + owned[:, hidden + 1 : hidden + 2]
        scale = lax.rsqrt(total / D + EPSILON)
        gate = owned[:, :hidden] * scale
        up = owned[:, wide : wide + hidden] * scale
        act = (jax.nn.silu(gate) * up).astype(bf16)
        return sent_to_all(act, "z").reshape(half, hidden)

    def tp_summed(value, name):
        own, other = side[name]
        partial = jnp.concatenate([matmul(value, own), matmul(value, other)], axis=1)
        return jnp.sum(sent_to_all(partial.astype(bf16), "tp").astype(f32), axis=0)

    act = ff_hidden("gain0", ff_names[:2], True)
    summed = tp_summed(act, "pre_down")
    resid = (side["resid"].astype(f32) + 0.5 * summed).astype(bf16)
    side["resid"] = resid

    turned = jnp.concatenate([resid[:, own_cols:], resid[:, :own_cols]], axis=1)
    all_rows = jnp.concatenate([resid, lax.ppermute(turned, "c", swap)], axis=0)
    slot_rows = matmul(side["spread"], all_rows).astype(bf16)
    own, other = zip(*[side[name] for name in head_names], strict=True)
    product = products(slot_rows, side["gain1"], True, own, other, matmul)
    sent = jnp.concatenate([*product, squares_of(slot_rows, LANES)], axis=1).astype(bf16)
    sent = sent.reshape(z_count, seq_local * W, 4 * head_cols + LANES)
    side["states"] = states
    owned = jnp.sum(exchanged(sent, "z").astype(f32), axis=0)
    at = 4 * head_cols
    total = owned[:, at : at + 1] + owned[:, at + 1 : at + 2]
    owned = owned[:, :at] * lax.rsqrt(total / D + EPSILON)

    shape_four = (seq_local, W, heads_local, DK)
    queries = jax.nn.silu(owned[:, :head_cols]).reshape(shape_four)
    forget_raw = owned[:, head_cols : 2 * head_cols].reshape(shape_four)
    fresh_values = owned[:, 2 * head_cols : 3 * head_cols].reshape(shape_four)
    gating = owned[:, 3 * head_cols :].reshape(shape_four)
    live = side["live"]
    forgets = jnp.where(
        live > 0, side["floors"] + side["rises"] * jax.nn.sigmoid(forget_raw), jnp.float32(1.0)
    )
    write_rate = 1.0 - forgets
    carried = side["states"]
    readings = []
    for offset in range(W):
        carried = (
            forgets[:, offset, :, :, None] * carried
            + write_rate[:, offset, :, :, None] * fresh_values[:, offset, :, None, :]
        )
        readings.append(jnp.sum(queries[:, offset, :, :, None] * carried, axis=2))
    side["states"] = carried
    read_out = jnp.stack(readings, axis=1)
    meansq = jnp.mean(read_out * read_out, axis=3, keepdims=True)
    head_out = (
        read_out * lax.rsqrt(meansq + EPSILON) * head_gain * jax.nn.silu(gating) * live
    ).astype(bf16)
    head_out = head_out.reshape(seq_local * W, heads_local * DK)
    all_heads = sent_to_all(head_out, ("z", "c")).reshape(slot_count, heads_local * DK)
    head_rows = matmul(side["my_table"], all_heads).astype(bf16)
    summed = tp_summed(head_rows, "mix")
    side["resid"] = (side["resid"].astype(f32) + summed).astype(bf16)

    act = ff_hidden("gain2", ff_names[2:], False)
    contract = (((0,), (1,)), ((), ()))
    finish = jnp.stack(
        [
            lax.dot_general(down, act, contract, preferred_element_type=f32)
            for down in side["post_down"]
        ]
    )
    first = (lax.axis_index("tp") == 0).astype(f32)
    residual = side["resid"].astype(f32).T.reshape(2, own_cols, half)
    finish = 0.5 * finish + first * residual
    finish = jnp.where(core == 0, finish, finish[::-1])
    finish = finish.reshape(2 * tp_count, own_cols // tp_count, half)
    finished = jnp.sum(exchanged(finish, ("c", "tp")).reshape(2, tp_count, -1, half), axis=1)
    finished = jnp.concatenate([finished[0], finished[1]], axis=1).astype(bf16)
    outcome = lax.dot_general(
        side["table"], finished, (((0,), (1,)), ((), ())), preferred_element_type=f32
    ).astype(bf16)
    return (outcome, side["states"])


def solution(mesh):
    kv = mesh.shape["kv"]
    tp = mesh.shape["tp"]
    cut = Mesh(mesh.devices.reshape(kv // 2, 2, tp), ("z", "c", "tp"))
    kv_axes = ("z", "c")
    placed = (
        P(None, ("z", "c", "tp")),
        P(),
        P(kv_axes, "tp", None, None),
        P(kv_axes),
        P(kv_axes, "tp"),
        P(kv_axes, "tp"),
        P("tp", kv_axes),
        P(kv_axes),
        P(kv_axes, "tp"),
        P(kv_axes, "tp"),
        P(kv_axes, "tp"),
        P(kv_axes, "tp"),
        P("tp"),
        P(),
        P("tp", kv_axes),
        P(kv_axes),
        P(kv_axes, "tp"),
        P(kv_axes, "tp"),
        P("tp", kv_axes),
    )
    return jax.shard_map(
        local,
        mesh=cut,
        in_specs=placed,
        out_specs=(P(None, ("z", "c", "tp")), P(kv_axes, "tp", None, None)),
        check_vma=False,
    )
```

```python
import jax
import jax.numpy as jnp
from jax import lax
from jax.experimental import pallas as pl
from jax.experimental.pallas import tpu as pltpu
from jax.sharding import Mesh
from jax.sharding import PartitionSpec as P

D = 4096
DK = 128
W = 4
EPSILON = 1e-06
LANES = 128
GAIN_ROWS = 16

f32 = jnp.float32
bf16 = jnp.bfloat16
barrier = lax.optimization_barrier


def matmul(a, b):
    return jnp.dot(a, b, preferred_element_type=f32)


def matmul_t(a, b):
    return lax.dot_general(a, b, (((1,), (1,)), ((), ())), preferred_element_type=f32)


def pack_kernel(*refs):
    weights, gains, out, sems = refs[:-5], refs[-5:-2], refs[-2], refs[-1]
    copies = []
    at = 0
    for i, ref in enumerate(weights):
        count = ref.shape[0]
        copies.append(pltpu.make_async_copy(ref, out.at[pl.ds(at, count)], sems.at[i]))
        copies[-1].start()
        at += count
    pieces = []
    for ref in gains:
        value = ref[...]
        high = value.astype(bf16).astype(f32)
        rest = value - high
        mid = rest.astype(bf16).astype(f32)
        pieces += [high, mid, rest - mid]
    pieces.append(jnp.zeros((GAIN_ROWS - len(pieces), LANES), f32))
    out[at:, :] = jnp.concatenate(pieces, axis=0).astype(bf16)
    for copy in copies:
        copy.wait()


def packed_weights(weights, gains):
    rows = sum(w.shape[0] for w in weights) + GAIN_ROWS
    return pl.pallas_call(
        pack_kernel,
        in_specs=[pl.BlockSpec(memory_space=pl.ANY)] * len(weights)
        + [pl.BlockSpec(memory_space=pltpu.VMEM)] * len(gains),
        out_specs=pl.BlockSpec(memory_space=pltpu.VMEM),
        out_shape=pltpu.VMEM((rows, weights[0].shape[1]), bf16),
        scratch_shapes=[pltpu.SemaphoreType.DMA((len(weights),))],
    )(*weights, *[gain[None, :] for gain in gains])


def squares_of(rows, lanes):
    wide = rows.astype(f32)
    total = jnp.sum(wide * wide, axis=1, keepdims=True)
    high = lax.reduce_precision(total, 8, 7)
    return jnp.where(lanes == 0, high, jnp.where(lanes == 1, total - high, 0.0))


def slot_targets(lengths, slot_count):
    seq_count = lengths.shape[0]
    seqs = jnp.arange(seq_count, dtype=jnp.int32)
    slots = jnp.arange(slot_count, dtype=jnp.int32)
    seq_of = slots // W
    within = slots % W
    before = jnp.sum(jnp.where(seqs[None, :] < seq_of[:, None], lengths[None, :], 0), axis=1)
    own = jnp.sum(jnp.where(seqs[None, :] == seq_of[:, None], lengths[None, :], 0), axis=1)
    return jnp.where(within < own, before + within, -1)


def products(rows, gain, exact, weights, product):
    count = rows.shape[0]
    wide = rows.astype(f32) * gain
    if not exact:
        return product(wide.astype(bf16), weights)
    rest = wide - lax.reduce_precision(wide, 8, 7)
    both = product(jnp.concatenate([wide, rest], axis=0).astype(bf16), weights)
    return both[:count] + both[count:]


def local(
    tokens,
    lengths,
    states,
    gain_pre,
    pre_gate,
    pre_up,
    pre_down,
    gain_mix,
    query_weight,
    forget_weight,
    input_weight,
    outgate_weight,
    forget_floor,
    head_gain,
    mix_weight,
    gain_post,
    post_gate,
    post_up,
    post_down,
):
    core = lax.axis_index("c")
    z_count = lax.axis_size("z")
    tp_count = lax.axis_size("tp")
    slot_count = tokens.shape[0]
    packed = slot_count // 2
    half = packed // 2
    per_z = half // z_count
    own_cols = gain_pre.shape[0]
    hidden = pre_gate.shape[1]
    ff_cols = 2 * hidden
    head_cols = query_weight.shape[1]
    seq_local, heads_local = states.shape[:2]
    swap = [(0, 1), (1, 0)]

    side = {}

    def exchanged(value, axis):
        value, tied = barrier((value, dict(side)))
        value = lax.all_to_all(value, axis, split_axis=0, concat_axis=0, tiled=True)
        value, tied = barrier((value, tied))
        side.update(tied)
        return value

    def sent_to_all(value, axis):
        return exchanged(jnp.broadcast_to(value, (lax.axis_size(axis), *value.shape)), axis)

    mine = (pre_gate.T, pre_up.T, post_gate.T, post_up.T)
    mine += (query_weight, forget_weight, input_weight, outgate_weight)
    mine += (mix_weight, pre_down, post_down)
    gains = (gain_pre, gain_mix, gain_post)
    bundle = lax.ppermute(packed_weights(mine, gains), "c", swap)

    targets = slot_targets(lengths, slot_count)
    rows = jnp.arange(packed, dtype=jnp.int32)
    table = (rows[:, None] == targets[None, :]).astype(bf16)
    row_ids = jnp.where(core == 0, rows, (rows + half) % packed)
    by_owner = targets.reshape(z_count, 2, seq_local * W)
    own_targets = jnp.where(core == 0, by_owner[:, 0], by_owner[:, 1]).reshape(packed)
    first_seq = (lax.axis_index("z") * 2 + core) * seq_local
    local_lengths = lax.dynamic_slice_in_dim(lengths, first_seq, seq_local)
    live = jnp.arange(W, dtype=jnp.int32)[None, :] < local_lengths[:, None]
    side["table"] = table
    side["my_table"] = jnp.where(core == 0, table[:half], table[half:])
    side["spread"] = (own_targets[:, None] == row_ids[None, :]).astype(bf16)
    side["live"] = live[:, :, None, None].astype(f32)
    side["floors"] = forget_floor.reshape(heads_local, DK)
    side["rises"] = 1.0 - side["floors"]
    side["first"] = (lax.axis_index("tp") == 0).astype(f32)
    side["lanes"] = lax.broadcasted_iota(jnp.int32, (1, LANES), 1)

    entry = lax.dot_general(
        tokens, table, (((0,), (1,)), ((), ())), preferred_element_type=f32
    ).astype(bf16)
    pieces = jnp.stack([entry[:, :half], entry[:, half:]])
    pieces = jnp.broadcast_to(pieces[:, None], (2, tp_count, *pieces.shape[1:]))
    gathered = exchanged(pieces.reshape(2 * tp_count, *pieces.shape[2:]), ("c", "tp"))
    gathered = gathered.reshape(2, own_cols, half)
    gathered = jnp.where(core == 0, gathered, gathered[::-1])
    side["resid"] = gathered.reshape(2 * own_cols, half).T

    theirs = []
    at = 0
    for weight in mine:
        theirs.append(bundle[at : at + weight.shape[0]])
        at += weight.shape[0]
    parts = bundle[at : at + 3 * len(gains)].astype(f32)
    for i, gain in enumerate(gains):
        other = jnp.sum(parts[3 * i : 3 * i + 3], axis=0)
        side[f"gain{i}"] = jnp.concatenate([gain, other])[None, :]
    for i, name in ((0, "pre_ff"), (2, "post_ff")):
        side[name] = [[mine[i], theirs[i]], [mine[i + 1], theirs[i + 1]]]
    side["heads"] = [list(mine[4:8]), theirs[4:8]]
    for i, name in ((8, "mix"), (9, "pre_down"), (10, "post_down")):
        side[name] = (mine[i], theirs[i])

    def ff_hidden(gain, name, exact):
        resid = side["resid"]
        product = products(resid, side[gain], exact, jnp.block(side[name]), matmul_t)
        sent = jnp.concatenate([product, squares_of(resid, side["lanes"])], axis=1)
        sent = sent.astype(bf16).reshape(z_count, per_z, ff_cols + LANES)
        owned = jnp.sum(exchanged(sent, "z").astype(f32), axis=0)
        total = owned[:, ff_cols : ff_cols + 1] + owned[:, ff_cols + 1 : ff_cols + 2]
        scale = lax.rsqrt(total / D + EPSILON)
        gate = owned[:, :hidden] * scale
        up = owned[:, hidden:ff_cols] * scale
        act = (jax.nn.silu(gate) * up).astype(bf16)
        return sent_to_all(act, "z").reshape(half, hidden)

    def tp_summed(value, name):
        own, other = side[name]
        partial = jnp.concatenate([matmul(value, own), matmul(value, other)], axis=1)
        return jnp.sum(sent_to_all(partial.astype(bf16), "tp").astype(f32), axis=0)

    act = ff_hidden("gain0", "pre_ff", True)
    summed = tp_summed(act, "pre_down")
    resid = (side["resid"].astype(f32) + 0.5 * summed).astype(bf16)
    side["resid"] = resid

    turned = jnp.concatenate([resid[:, own_cols:], resid[:, :own_cols]], axis=1)
    all_rows = jnp.concatenate([resid, lax.ppermute(turned, "c", swap)], axis=0)
    slot_rows = matmul(side["spread"], all_rows).astype(bf16)
    product = products(slot_rows, side["gain1"], True, jnp.block(side["heads"]), matmul)
    sent = jnp.concatenate([product, squares_of(slot_rows, side["lanes"])], axis=1).astype(bf16)
    sent = sent.reshape(z_count, seq_local * W, 4 * head_cols + LANES)
    side["states"] = states
    owned = jnp.sum(exchanged(sent, "z").astype(f32), axis=0)
    at = 4 * head_cols
    total = owned[:, at : at + 1] + owned[:, at + 1 : at + 2]
    owned = owned[:, :at] * lax.rsqrt(total / D + EPSILON)

    shape_four = (seq_local, W, heads_local, DK)
    queries = jax.nn.silu(owned[:, :head_cols]).reshape(shape_four)
    forget_raw = owned[:, head_cols : 2 * head_cols].reshape(shape_four)
    fresh_values = owned[:, 2 * head_cols : 3 * head_cols].reshape(shape_four)
    gating = owned[:, 3 * head_cols :].reshape(shape_four)
    live = side["live"]
    forgets = jnp.where(
        live > 0, side["floors"] + side["rises"] * jax.nn.sigmoid(forget_raw), jnp.float32(1.0)
    )
    write_rate = 1.0 - forgets
    carried = side["states"]
    readings = []
    for offset in range(W):
        carried = (
            forgets[:, offset, :, :, None] * carried
            + write_rate[:, offset, :, :, None] * fresh_values[:, offset, :, None, :]
        )
        readings.append(jnp.sum(queries[:, offset, :, :, None] * carried, axis=2))
    side["states"] = carried
    read_out = jnp.stack(readings, axis=1)
    meansq = jnp.mean(read_out * read_out, axis=3, keepdims=True)
    head_out = (
        read_out * lax.rsqrt(meansq + EPSILON) * head_gain * jax.nn.silu(gating) * live
    ).astype(bf16)
    head_out = head_out.reshape(seq_local * W, heads_local * DK)
    all_heads = sent_to_all(head_out, ("z", "c")).reshape(slot_count, heads_local * DK)
    head_rows = matmul(side["my_table"], all_heads).astype(bf16)
    summed = tp_summed(head_rows, "mix")
    side["resid"] = (side["resid"].astype(f32) + summed).astype(bf16)

    act = ff_hidden("gain2", "post_ff", False)
    contract = (((0,), (1,)), ((), ()))
    finish = jnp.stack(
        [
            lax.dot_general(down, act, contract, preferred_element_type=f32)
            for down in side["post_down"]
        ]
    )
    residual = side["resid"].astype(f32).T.reshape(2, own_cols, half)
    finish = 0.5 * finish + side["first"] * residual
    finish = jnp.where(core == 0, finish, finish[::-1])
    piece = own_cols // tp_count
    finish = finish.reshape(2 * tp_count, piece * half)
    finished = jnp.sum(exchanged(finish, ("c", "tp")).reshape(2, tp_count, -1), axis=1)
    finished = finished.reshape(2, piece, half)
    finished = jnp.concatenate([finished[0], finished[1]], axis=1).astype(bf16)
    outcome = matmul(finished, side["table"]).astype(bf16).T
    return (outcome, side["states"])


def solution(mesh):
    kv = mesh.shape["kv"]
    tp = mesh.shape["tp"]
    cut = Mesh(mesh.devices.reshape(kv // 2, 2, tp), ("z", "c", "tp"))
    kv_axes = ("z", "c")
    placed = (
        P(None, ("z", "c", "tp")),
        P(),
        P(kv_axes, "tp", None, None),
        P(kv_axes),
        P(kv_axes, "tp"),
        P(kv_axes, "tp"),
        P("tp", kv_axes),
        P(kv_axes),
        P(kv_axes, "tp"),
        P(kv_axes, "tp"),
        P(kv_axes, "tp"),
        P(kv_axes, "tp"),
        P("tp"),
        P(),
        P("tp", kv_axes),
        P(kv_axes),
        P(kv_axes, "tp"),
        P(kv_axes, "tp"),
        P("tp", kv_axes),
    )
    return jax.shard_map(
        local,
        mesh=cut,
        in_specs=placed,
        out_specs=(P(None, ("z", "c", "tp")), P(kv_axes, "tp", None, None)),
        check_vma=False,
    )
```

```python
import functools

import jax
import jax.numpy as jnp
from jax import lax
from jax.experimental import pallas as pl
from jax.experimental.pallas import tpu as pltpu
from jax.sharding import Mesh
from jax.sharding import PartitionSpec as P

D = 4096
DK = 128
W = 4
EPSILON = 1e-06
LANES = 128
GAIN_ROWS = 16

f32 = jnp.float32
bf16 = jnp.bfloat16
barrier = lax.optimization_barrier


def matmul(a, b):
    return jnp.dot(a, b, preferred_element_type=f32)


def in_vmem(value):
    return pltpu.with_memory_space_constraint(value, pltpu.VMEM)


def matmul_t(a, b):
    return lax.dot_general(a, b, (((1,), (1,)), ((), ())), preferred_element_type=f32)


def iota(shape, axis):
    return lax.broadcasted_iota(jnp.int32, shape, axis)


def tables_of(lengths, tokens, core):
    slots = tokens.shape[1]
    packed = slots // 2
    half = packed // 2
    seqs = lengths.shape[1]
    slot = iota((1, slots), 1)
    seq, seq_of = iota((seqs, slots), 0), iota((seqs, slots), 1) // W
    wide = jnp.broadcast_to(lengths, (8, seqs)).astype(bf16)
    before = matmul(wide, (seq < seq_of).astype(f32).astype(bf16))[:1]
    own = matmul(wide, (seq == seq_of).astype(f32).astype(bf16))[:1]
    within = (slot % W).astype(f32)
    targets = jnp.where(within < own, before + within, -1.0)
    rows = iota((packed, slots), 0).astype(f32)
    table = (rows == targets).astype(f32).astype(bf16)
    rows = (iota((half, slots), 0) + core * half).astype(f32)
    my_table = (rows == targets).astype(f32).astype(bf16)
    place = iota((packed, 1), 0)
    my_slot = place // 8 * 16 + core * 8 + place % 8
    before, own = counted(lengths, my_slot)
    within = (my_slot % W).astype(f32)
    targets = jnp.where(within < own, before + within, -1.0)
    row_ids = ((iota((1, packed), 1) + core * half) % packed).astype(f32)
    spread = (targets == row_ids).astype(f32).astype(bf16)
    entry = matmul_t(tokens, table).astype(bf16)
    return table, my_table, spread, entry


def counted(lengths, slots):
    seq = iota((slots.shape[0], lengths.shape[1]), 1)
    before = jnp.sum(jnp.where(seq < slots // W, lengths, 0.0), axis=1, keepdims=True)
    own = jnp.sum(jnp.where(seq == slots // W, lengths, 0.0), axis=1, keepdims=True)
    return before, own


def front_kernel(count, *refs):
    weights, gains, refs = refs[:count], refs[count : count + 3], refs[count + 3 :]
    lengths, tokens, out, table, my_table, spread, entry, sems = refs
    copies = []
    at = 0
    for i, ref in enumerate(weights):
        rows = ref.shape[0]
        copies.append(pltpu.make_async_copy(ref, out.at[pl.ds(at, rows)], sems.at[i]))
        copies[-1].start()
        at += rows
    pieces = []
    for ref in gains:
        value = ref[...]
        high = value.astype(bf16).astype(f32)
        rest = value - high
        mid = rest.astype(bf16).astype(f32)
        pieces += [high, mid, rest - mid]
    pieces.append(jnp.zeros((GAIN_ROWS - len(pieces), LANES), f32))
    out[at:, :] = jnp.concatenate(pieces, axis=0).astype(bf16)
    results = tables_of(lengths[...].astype(f32), tokens[...], lax.axis_index("c"))
    for ref, value in zip((table, my_table, spread, entry), results, strict=True):
        ref[...] = value
    for copy in copies:
        copy.wait()


def front(weights, gains, lengths, tokens):
    rows = sum(w.shape[0] for w in weights) + GAIN_ROWS
    slots = tokens.shape[1]
    packed = slots // 2
    shapes = (
        (rows, weights[0].shape[1]),
        (packed, slots),
        (packed // 2, slots),
        (packed, packed),
        (tokens.shape[0], packed),
    )
    vmem = pl.BlockSpec(memory_space=pltpu.VMEM)
    return pl.pallas_call(
        functools.partial(front_kernel, len(weights)),
        in_specs=[pl.BlockSpec(memory_space=pl.ANY)] * len(weights)
        + [vmem] * (len(gains) + 2),
        out_specs=[vmem] * len(shapes),
        out_shape=[pltpu.VMEM(shape, bf16) for shape in shapes],
        scratch_shapes=[pltpu.SemaphoreType.DMA((len(weights),))],
    )(*weights, *[gain[None, :] for gain in gains], lengths[None, :], tokens)


def recur_kernel(sums, lengths, floors, head_gain, states, heads, new_states, scratch, sems):
    total = jnp.sum(sums[...].astype(f32), axis=0)
    slots = total.shape[0]
    at = 4 * DK
    squares = total[:, at : at + 1] + total[:, at + 1 : at + 2]
    total = total[:, :at] * lax.rsqrt(squares / D + EPSILON)
    queries = total[:, :DK]
    queries = queries * jax.nn.sigmoid(queries)
    fresh = total[:, 2 * DK : 3 * DK]
    gating = total[:, 3 * DK :]
    first = (lax.axis_index("z") * 2 + lax.axis_index("c")) * slots
    slot = iota((slots, 1), 0) + first
    _, own = counted(lengths[...].astype(f32), slot)
    live = ((slot % W).astype(f32) < own).astype(f32)
    floor = floors[...]
    forgets = floor + (1.0 - floor) * jax.nn.sigmoid(total[:, DK : 2 * DK])
    forgets = jnp.where(live > 0, forgets, 1.0)
    both = jnp.concatenate([queries, forgets], axis=0).T
    readings, copies = [], []
    for seq in range(states.shape[0]):
        carried = states[seq]
        for offset in range(W):
            row = seq * W + offset
            query = both[:, row : row + 1]
            forget = both[:, slots + row : slots + row + 1]
            carried = forget * carried + (1.0 - forget) * fresh[row : row + 1]
            readings.append(jnp.sum(query * carried, axis=0, keepdims=True))
        scratch[seq] = carried
        copies.append(pltpu.make_async_copy(scratch.at[seq], new_states.at[seq], sems.at[seq]))
        copies[-1].start()
    read_out = jnp.concatenate(readings, axis=0)
    meansq = jnp.mean(read_out * read_out, axis=1, keepdims=True)
    gate = gating * jax.nn.sigmoid(gating)
    out = read_out * lax.rsqrt(meansq + EPSILON) * head_gain[...] * gate * live
    heads[...] = out.astype(bf16)
    for copy in copies:
        copy.wait()


def recurred(sums, lengths, floors, head_gain, states):
    vmem = pl.BlockSpec(memory_space=pltpu.VMEM)
    return pl.pallas_call(
        recur_kernel,
        in_specs=[vmem] * 5,
        out_specs=[vmem, pl.BlockSpec(memory_space=pl.ANY)],
        out_shape=[
            pltpu.VMEM((sums.shape[1], DK), bf16),
            jax.ShapeDtypeStruct(states.shape, f32),
        ],
        scratch_shapes=[
            pltpu.VMEM(states.shape, f32),
            pltpu.SemaphoreType.DMA((states.shape[0],)),
        ],
    )(*[in_vmem(value) for value in (sums, lengths, floors, head_gain, states)])


def gain_rows(bundle, which):
    at = bundle.shape[0] - GAIN_ROWS + 3 * which
    return jnp.sum(bundle[at : at + 3, :].astype(f32), axis=0, keepdims=True)


def stats_of(own, other):
    total = jnp.sum(own * own + other * other, axis=1, keepdims=True)
    upper = total.astype(bf16).astype(f32)
    lanes = iota((1, LANES), 1)
    return jnp.where(lanes == 0, upper, jnp.where(lanes == 1, total - upper, 0.0)).astype(bf16)


def products(sent, own, other, gains, weights, product, exact):
    parts = []
    for rows, gain in zip((own, other), gains, strict=True):
        wide = rows * gain
        whole = wide.astype(bf16)
        if exact:
            rest = (wide - whole.astype(f32)).astype(bf16)
            whole = jnp.concatenate([whole, rest], axis=0)
        parts.append(whole)
    count = own.shape[0]
    at = 0
    for ours, theirs in weights:
        both = product(parts[0], ours) + product(parts[1], theirs)
        if exact:
            both = both[:count] + both[count:]
        sent[:, at : at + both.shape[1]] = both.astype(bf16)
        at += both.shape[1]
    sent[:, at:] = stats_of(own, other)


def halves_of(weights, bundle, at):
    pairs = []
    for weight in weights:
        pairs.append((weight[...], bundle[at : at + weight.shape[0], :]))
        at += weight.shape[0]
    return pairs


def entry_kernel(gathered, gain, gate, up, bundle, sent, resid):
    cols = gain.shape[1]
    first = lax.axis_index("c") == 0
    low, high = gathered[:cols, :].astype(f32), gathered[cols:, :].astype(f32)
    own = jnp.where(first, low, high).T
    other = jnp.where(first, high, low).T
    resid[:, :cols] = own.astype(bf16)
    resid[:, cols:] = other.astype(bf16)
    weights = halves_of((gate, up), bundle, 0)
    gains = (gain[...], gain_rows(bundle, 0))
    products(sent, own, other, gains, weights, matmul_t, True)


def mix_kernel(spread, resid, swapped, gain, query, forget, value, outgate, bundle, at, sent):
    cols = gain.shape[1]
    rows = jnp.concatenate([resid[...], swapped[...]], axis=0)
    rows = matmul(spread[...], rows)
    weights = halves_of((query, forget, value, outgate), bundle, at)
    gains = (gain[...], gain_rows(bundle, 1))
    products(sent, rows[:, :cols], rows[:, cols:], gains, weights, matmul, True)


def post_kernel(received, before, gain, gate, up, bundle, at, sent, resid):
    cols = gain.shape[1]
    total = jnp.sum(received[...].astype(f32), axis=0)
    rows = (before[...].astype(f32) + total).astype(bf16)
    resid[...] = rows
    rows = rows.astype(f32)
    weights = halves_of((gate, up), bundle, at)
    gains = (gain[...], gain_rows(bundle, 2))
    products(sent, rows[:, :cols], rows[:, cols:], gains, weights, matmul_t, False)


def in_kernel(kernel, shapes, *values):
    vmem = pl.BlockSpec(memory_space=pltpu.VMEM)
    return pl.pallas_call(
        kernel,
        in_specs=[vmem] * len(values),
        out_specs=[vmem] * len(shapes),
        out_shape=[pltpu.VMEM(shape, bf16) for shape in shapes],
    )(*[in_vmem(value) for value in values])


def local(
    tokens,
    lengths,
    states,
    gain_pre,
    pre_gate,
    pre_up,
    pre_down,
    gain_mix,
    query_weight,
    forget_weight,
    input_weight,
    outgate_weight,
    forget_floor,
    head_gain,
    mix_weight,
    gain_post,
    post_gate,
    post_up,
    post_down,
):
    core = lax.axis_index("c")
    z_count = lax.axis_size("z")
    tp_count = lax.axis_size("tp")
    slot_count = tokens.shape[0]
    packed = slot_count // 2
    half = packed // 2
    per_z = half // z_count
    own_cols = gain_pre.shape[0]
    hidden = pre_gate.shape[1]
    ff_cols = 2 * hidden
    head_cols = query_weight.shape[1]
    seq_local, heads_local = states.shape[:2]
    swap = [(0, 1), (1, 0)]

    side = {}

    def exchanged(value, axis):
        value, tied = barrier((value, dict(side)))
        value = lax.all_to_all(value, axis, split_axis=0, concat_axis=0, tiled=True)
        value, tied = barrier((value, tied))
        side.update(tied)
        return value

    def sent_to_all(value, axis):
        return exchanged(jnp.broadcast_to(value, (lax.axis_size(axis), *value.shape)), axis)

    mine = (pre_gate.T, pre_up.T, post_gate.T, post_up.T)
    mine += (query_weight, forget_weight, input_weight, outgate_weight)
    mine += (mix_weight, pre_down, post_down)
    gains = (gain_pre, gain_mix, gain_post)
    packed_own, table, my_table, spread, entry = front(mine, gains, lengths, tokens.T)
    bundle = lax.ppermute(packed_own, "c", swap)

    side["table"] = table
    side["my_table"] = my_table
    side["spread"] = spread
    side["core"] = core
    side["first"] = (lax.axis_index("tp") == 0).astype(f32)

    pieces = jnp.stack([entry[:, :half], entry[:, half:]])
    pieces = jnp.broadcast_to(pieces[:, None], (2, tp_count, *pieces.shape[1:]))
    gathered = exchanged(pieces.reshape(2 * tp_count, *pieces.shape[2:]), ("c", "tp"))
    starts = [0]
    for weight in mine:
        starts.append(starts[-1] + weight.shape[0])

    def other(i):
        return side["bundle"][starts[i] : starts[i + 1]]

    side["bundle"] = bundle
    sent_shape = (half, ff_cols + LANES)
    resid_shape = (half, 2 * own_cols)
    sent, side["resid"] = in_kernel(
        entry_kernel,
        (sent_shape, resid_shape),
        gathered.reshape(2 * own_cols, half),
        gain_pre[None, :],
        mine[0],
        mine[1],
        bundle,
    )

    def ff_hidden(sent):
        sent = sent.reshape(z_count, per_z, ff_cols + LANES)
        owned = jnp.sum(exchanged(sent, "z").astype(f32), axis=0)
        total = owned[:, ff_cols : ff_cols + 1] + owned[:, ff_cols + 1 : ff_cols + 2]
        scale = lax.rsqrt(total / D + EPSILON)
        gate = owned[:, :hidden] * scale
        up = owned[:, hidden:ff_cols] * scale
        act = (jax.nn.silu(gate) * up).astype(bf16)
        return sent_to_all(act, "z").reshape(half, hidden)

    def tp_partials(value, i):
        partial = jnp.concatenate([matmul(value, mine[i]), matmul(value, other(i))], axis=1)
        return sent_to_all(partial.astype(bf16), "tp")

    act = ff_hidden(sent)
    summed = jnp.sum(tp_partials(act, 9).astype(f32), axis=0)
    resid = (side["resid"].astype(f32) + 0.5 * summed).astype(bf16)
    side["resid"] = resid

    turned = jnp.concatenate([resid[:, own_cols:], resid[:, :own_cols]], axis=1)
    swapped = lax.ppermute(turned, "c", swap)
    (sent,) = in_kernel(
        lambda *refs: mix_kernel(*refs[:-1], starts[4], refs[-1]),
        ((packed, 4 * head_cols + LANES),),
        side["spread"],
        resid,
        swapped,
        gain_mix[None, :],
        *mine[4:8],
        side["bundle"],
    )
    sent = sent.reshape(z_count, seq_local * W, 4 * head_cols + LANES)
    side["recur"] = (lengths[None, :], forget_floor[None, :], head_gain[None, :])
    side["states"] = states.reshape(seq_local * heads_local, DK, DK)
    received = exchanged(sent, "z")
    head_out, new_states = recurred(received, *side.pop("recur"), side.pop("states"))
    all_heads = sent_to_all(head_out, ("z", "c")).reshape(slot_count, DK)
    head_rows = matmul(side["my_table"], all_heads).astype(bf16)
    sent, side["resid"] = in_kernel(
        lambda *refs: post_kernel(*refs[:-2], starts[2], *refs[-2:]),
        (sent_shape, resid_shape),
        tp_partials(head_rows, 8),
        side["resid"],
        gain_post[None, :],
        mine[2],
        mine[3],
        side["bundle"],
    )
    act = ff_hidden(sent)
    contract = (((0,), (1,)), ((), ()))
    finish = jnp.stack(
        [
            lax.dot_general(down, act, contract, preferred_element_type=f32)
            for down in (post_down, other(10))
        ]
    )
    residual = side["resid"].astype(f32).T.reshape(2, own_cols, half)
    finish = 0.5 * finish + side["first"] * residual
    finish = jnp.where(side["core"] == 0, finish, finish[::-1])
    piece = own_cols // tp_count
    finish = finish.reshape(2 * tp_count, piece * half)
    finished = jnp.sum(exchanged(finish, ("c", "tp")).reshape(2, tp_count, -1), axis=1)
    finished = finished.reshape(2, piece, half)
    finished = jnp.concatenate([finished[0], finished[1]], axis=1).astype(bf16)
    outcome = matmul(finished, side["table"]).astype(bf16).T
    return (outcome, new_states.reshape(states.shape))


def solution(mesh):
    kv = mesh.shape["kv"]
    tp = mesh.shape["tp"]
    cut = Mesh(mesh.devices.reshape(kv // 2, 2, tp), ("z", "c", "tp"))
    kv_axes = ("z", "c")
    placed = (
        P(None, ("z", "c", "tp")),
        P(),
        P(kv_axes, "tp", None, None),
        P(kv_axes),
        P(kv_axes, "tp"),
        P(kv_axes, "tp"),
        P("tp", kv_axes),
        P(kv_axes),
        P(kv_axes, "tp"),
        P(kv_axes, "tp"),
        P(kv_axes, "tp"),
        P(kv_axes, "tp"),
        P("tp"),
        P(),
        P("tp", kv_axes),
        P(kv_axes),
        P(kv_axes, "tp"),
        P(kv_axes, "tp"),
        P("tp", kv_axes),
    )
    return jax.shard_map(
        local,
        mesh=cut,
        in_specs=placed,
        out_specs=(P(None, ("z", "c", "tp")), P(kv_axes, "tp", None, None)),
        check_vma=False,
    )
```

```python
import functools

import jax
import jax.numpy as jnp
from jax import lax
from jax.experimental import pallas as pl
from jax.experimental.pallas import tpu as pltpu
from jax.sharding import Mesh
from jax.sharding import PartitionSpec as P

D = 4096
DK = 128
W = 4
EPSILON = 1e-06
LANES = 128
GAIN_ROWS = 16

f32 = jnp.float32
bf16 = jnp.bfloat16
barrier = lax.optimization_barrier
SMALL = pltpu.CompilerParams(vmem_limit_bytes=16 * 2**20)


def matmul(a, b):
    return jnp.dot(a, b, preferred_element_type=f32)


def in_vmem(value):
    return pltpu.with_memory_space_constraint(value, pltpu.VMEM)


def matmul_t(a, b):
    return lax.dot_general(a, b, (((1,), (1,)), ((), ())), preferred_element_type=f32)


def iota(shape, axis):
    return lax.broadcasted_iota(jnp.int32, shape, axis)


def tables_of(lengths, tokens, core):
    slots = tokens.shape[1]
    packed = slots // 2
    half = packed // 2
    seqs = lengths.shape[1]
    slot = iota((1, slots), 1)
    seq, seq_of = iota((seqs, slots), 0), iota((seqs, slots), 1) // W
    wide = jnp.broadcast_to(lengths, (8, seqs)).astype(bf16)
    before = matmul(wide, (seq < seq_of).astype(f32).astype(bf16))[:1]
    own = matmul(wide, (seq == seq_of).astype(f32).astype(bf16))[:1]
    within = (slot % W).astype(f32)
    targets = jnp.where(within < own, before + within, -1.0)
    rows = iota((packed, slots), 0).astype(f32)
    table = (rows == targets).astype(f32).astype(bf16)
    rows = (iota((half, slots), 0) + core * half).astype(f32)
    my_table = (rows == targets).astype(f32).astype(bf16)
    place = iota((packed, 1), 0)
    my_slot = place // 8 * 16 + core * 8 + place % 8
    before, own = counted(lengths, my_slot)
    within = (my_slot % W).astype(f32)
    targets = jnp.where(within < own, before + within, -1.0)
    row_ids = ((iota((1, packed), 1) + core * half) % packed).astype(f32)
    spread = (targets == row_ids).astype(f32).astype(bf16)
    entry = matmul_t(tokens, table).astype(bf16)
    return table, my_table, spread, entry


def counted(lengths, slots):
    seq = iota((slots.shape[0], lengths.shape[1]), 1)
    before = jnp.sum(jnp.where(seq < slots // W, lengths, 0.0), axis=1, keepdims=True)
    own = jnp.sum(jnp.where(seq == slots // W, lengths, 0.0), axis=1, keepdims=True)
    return before, own


def front_kernel(count, *refs):
    weights, gains, refs = refs[:count], refs[count : count + 3], refs[count + 3 :]
    lengths, tokens, out, table, my_table, spread, entry, sems = refs
    copies = []
    at = 0
    for i, ref in enumerate(weights):
        rows = ref.shape[0]
        copies.append(pltpu.make_async_copy(ref, out.at[pl.ds(at, rows)], sems.at[i]))
        copies[-1].start()
        at += rows
    pieces = []
    for ref in gains:
        value = ref[...]
        high = value.astype(bf16).astype(f32)
        rest = value - high
        mid = rest.astype(bf16).astype(f32)
        pieces += [high, mid, rest - mid]
    pieces.append(jnp.zeros((GAIN_ROWS - len(pieces), LANES), f32))
    out[at:, :] = jnp.concatenate(pieces, axis=0).astype(bf16)
    results = tables_of(lengths[...].astype(f32), tokens[...], lax.axis_index("c"))
    for ref, value in zip((table, my_table, spread, entry), results, strict=True):
        ref[...] = value
    for copy in copies:
        copy.wait()


def front(weights, gains, lengths, tokens):
    rows = sum(w.shape[0] for w in weights) + GAIN_ROWS
    slots = tokens.shape[1]
    packed = slots // 2
    shapes = (
        (rows, weights[0].shape[1]),
        (packed, slots),
        (packed // 2, slots),
        (packed, packed),
        (tokens.shape[0], packed),
    )
    vmem = pl.BlockSpec(memory_space=pltpu.VMEM)
    return pl.pallas_call(
        functools.partial(front_kernel, len(weights)),
        in_specs=[pl.BlockSpec(memory_space=pl.ANY)] * len(weights)
        + [vmem] * (len(gains) + 2),
        out_specs=[vmem] * len(shapes),
        out_shape=[pltpu.VMEM(shape, bf16) for shape in shapes],
        scratch_shapes=[pltpu.SemaphoreType.DMA((len(weights),))],
    )(*weights, *[gain[None, :] for gain in gains], lengths[None, :], tokens)


def recur_kernel(sums, lengths, floors, head_gain, states, heads, new_states):
    total = jnp.sum(sums[...].astype(f32), axis=0)
    slots = total.shape[0]
    at = 4 * DK
    squares = total[:, at : at + 1] + total[:, at + 1 : at + 2]
    total = total[:, :at] * lax.rsqrt(squares / D + EPSILON)
    queries = total[:, :DK]
    queries = queries * jax.nn.sigmoid(queries)
    fresh = total[:, 2 * DK : 3 * DK]
    gating = total[:, 3 * DK :]
    first = (lax.axis_index("z") * 2 + lax.axis_index("c")) * slots
    slot = iota((slots, 1), 0) + first
    _, own = counted(lengths[...].astype(f32), slot)
    live = ((slot % W).astype(f32) < own).astype(f32)
    floor = floors[...]
    forgets = floor + (1.0 - floor) * jax.nn.sigmoid(total[:, DK : 2 * DK])
    forgets = jnp.where(live > 0, forgets, 1.0)
    both = jnp.concatenate([queries, forgets], axis=0).T
    readings = []
    for seq in range(states.shape[0]):
        carried = states[seq]
        for offset in range(W):
            row = seq * W + offset
            query = both[:, row : row + 1]
            forget = both[:, slots + row : slots + row + 1]
            carried = forget * carried + (1.0 - forget) * fresh[row : row + 1]
            readings.append(jnp.sum(query * carried, axis=0, keepdims=True))
        new_states[seq] = carried
    read_out = jnp.concatenate(readings, axis=0)
    meansq = jnp.mean(read_out * read_out, axis=1, keepdims=True)
    gate = gating * jax.nn.sigmoid(gating)
    out = read_out * lax.rsqrt(meansq + EPSILON) * head_gain[...] * gate * live
    heads[...] = out.astype(bf16)


def recurred(sums, lengths, floors, head_gain, states):
    vmem = pl.BlockSpec(memory_space=pltpu.VMEM)
    return pl.pallas_call(
        recur_kernel,
        in_specs=[vmem] * 5,
        out_specs=[vmem, vmem],
        out_shape=[pltpu.VMEM((sums.shape[1], DK), bf16), pltpu.VMEM(states.shape, f32)],
        compiler_params=SMALL,
    )(*[in_vmem(value) for value in (sums, lengths, floors, head_gain, states)])


def gain_rows(bundle, which):
    at = bundle.shape[0] - GAIN_ROWS + 3 * which
    return jnp.sum(bundle[at : at + 3, :].astype(f32), axis=0, keepdims=True)


def stats_of(own, other):
    total = jnp.sum(own * own + other * other, axis=1, keepdims=True)
    upper = total.astype(bf16).astype(f32)
    lanes = iota((1, LANES), 1)
    return jnp.where(lanes == 0, upper, jnp.where(lanes == 1, total - upper, 0.0)).astype(bf16)


def products(sent, own, other, gains, weights, product, exact):
    parts = []
    for rows, gain in zip((own, other), gains, strict=True):
        wide = rows * gain
        whole = wide.astype(bf16)
        if exact:
            rest = (wide - whole.astype(f32)).astype(bf16)
            whole = jnp.concatenate([whole, rest], axis=0)
        parts.append(whole)
    count = own.shape[0]
    at = 0
    for ours, theirs in weights:
        both = product(parts[0], ours) + product(parts[1], theirs)
        if exact:
            both = both[:count] + both[count:]
        sent[:, at : at + both.shape[1]] = both.astype(bf16)
        at += both.shape[1]
    sent[:, at:] = stats_of(own, other)


def halves_of(weights, bundle, at):
    pairs = []
    for weight in weights:
        pairs.append((weight[...], bundle[at : at + weight.shape[0], :]))
        at += weight.shape[0]
    return pairs


def entry_kernel(gathered, gain, gate, up, bundle, sent, resid):
    cols = gain.shape[1]
    first = lax.axis_index("c") == 0
    low, high = gathered[:cols, :].astype(f32), gathered[cols:, :].astype(f32)
    own = jnp.where(first, low, high).T
    other = jnp.where(first, high, low).T
    resid[:, :cols] = own.astype(bf16)
    resid[:, cols:] = other.astype(bf16)
    weights = halves_of((gate, up), bundle, 0)
    gains = (gain[...], gain_rows(bundle, 0))
    products(sent, own, other, gains, weights, matmul_t, True)


def mix_kernel(spread, resid, swapped, gain, query, forget, value, outgate, bundle, at, sent):
    cols = gain.shape[1]
    rows = jnp.concatenate([resid[...], swapped[...]], axis=0)
    rows = matmul(spread[...], rows)
    weights = halves_of((query, forget, value, outgate), bundle, at)
    gains = (gain[...], gain_rows(bundle, 1))
    products(sent, rows[:, :cols], rows[:, cols:], gains, weights, matmul, True)


def post_kernel(received, before, gain, gate, up, bundle, at, sent, resid):
    cols = gain.shape[1]
    total = jnp.sum(received[...].astype(f32), axis=0)
    rows = (before[...].astype(f32) + total).astype(bf16)
    resid[...] = rows
    rows = rows.astype(f32)
    weights = halves_of((gate, up), bundle, at)
    gains = (gain[...], gain_rows(bundle, 2))
    products(sent, rows[:, :cols], rows[:, cols:], gains, weights, matmul_t, False)


def put_partials(rows, weight, other, out):
    cols = weight.shape[1]
    own = matmul(rows, weight[...]).astype(bf16)
    other = matmul(rows, other).astype(bf16)
    for i in range(out.shape[0]):
        out[i, :, :cols] = own
        out[i, :, cols:] = other


def down_kernel(rows, weight, bundle, at, out):
    put_partials(rows[...], weight, bundle[at : at + weight.shape[0], :], out)


def heads_kernel(heads, table, weight, states, bundle, at, out, new_states, sem):
    copy = pltpu.make_async_copy(states, new_states, sem)
    copy.start()
    rows = matmul(table[...], heads[...]).astype(bf16)
    put_partials(rows, weight, bundle[at : at + weight.shape[0], :], out)
    copy.wait()


def head_partials(heads, table, weight, states, bundle, at, shape):
    vmem = pl.BlockSpec(memory_space=pltpu.VMEM)
    values = [in_vmem(value) for value in (heads, table, weight, states, bundle)]
    return pl.pallas_call(
        lambda *refs: heads_kernel(*refs[:5], at, *refs[5:]),
        in_specs=[vmem] * len(values),
        out_specs=[vmem, pl.BlockSpec(memory_space=pl.ANY)],
        out_shape=[pltpu.VMEM(shape, bf16), jax.ShapeDtypeStruct(states.shape, f32)],
        scratch_shapes=[pltpu.SemaphoreType.DMA],
        compiler_params=SMALL,
    )(*values)


def finish_kernel(rows, resid, weight, bundle, at, out):
    cols = weight.shape[1]
    first = (lax.axis_index("tp") == 0).astype(f32)
    own = 0.5 * matmul(rows[...], weight[...]) + first * resid[:, :cols].astype(f32)
    other = matmul(rows[...], bundle[at : at + weight.shape[0], :])
    other = 0.5 * other + first * resid[:, cols:].astype(f32)
    own, other = own.T, other.T
    leads = lax.axis_index("c") == 0
    out[:cols, :] = jnp.where(leads, own, other)
    out[cols:, :] = jnp.where(leads, other, own)


def in_kernel(kernel, shapes, *values, dtype=bf16):
    vmem = pl.BlockSpec(memory_space=pltpu.VMEM)
    return pl.pallas_call(
        kernel,
        in_specs=[vmem] * len(values),
        out_specs=[vmem] * len(shapes),
        out_shape=[pltpu.VMEM(shape, dtype) for shape in shapes],
        compiler_params=SMALL,
    )(*[in_vmem(value) for value in values])


def local(
    tokens,
    lengths,
    states,
    gain_pre,
    pre_gate,
    pre_up,
    pre_down,
    gain_mix,
    query_weight,
    forget_weight,
    input_weight,
    outgate_weight,
    forget_floor,
    head_gain,
    mix_weight,
    gain_post,
    post_gate,
    post_up,
    post_down,
):
    z_count = lax.axis_size("z")
    tp_count = lax.axis_size("tp")
    slot_count = tokens.shape[0]
    packed = slot_count // 2
    half = packed // 2
    per_z = half // z_count
    own_cols = gain_pre.shape[0]
    hidden = pre_gate.shape[1]
    ff_cols = 2 * hidden
    head_cols = query_weight.shape[1]
    seq_local, heads_local = states.shape[:2]
    swap = [(0, 1), (1, 0)]

    side = {}

    def exchanged(value, axis):
        value, tied = barrier((value, dict(side)))
        value = lax.all_to_all(value, axis, split_axis=0, concat_axis=0, tiled=True)
        value, tied = barrier((value, tied))
        side.update(tied)
        return value

    def sent_to_all(value, axis):
        return exchanged(jnp.broadcast_to(value, (lax.axis_size(axis), *value.shape)), axis)

    mine = (pre_gate.T, pre_up.T, post_gate.T, post_up.T)
    mine += (query_weight, forget_weight, input_weight, outgate_weight)
    mine += (mix_weight, pre_down, post_down)
    gains = (gain_pre, gain_mix, gain_post)
    packed_own, table, my_table, spread, entry = front(mine, gains, lengths, tokens.T)
    bundle = lax.ppermute(packed_own, "c", swap)

    side["table"] = table
    side["my_table"] = my_table
    side["spread"] = spread

    pieces = jnp.stack([entry[:, :half], entry[:, half:]])
    pieces = jnp.broadcast_to(pieces[:, None], (2, tp_count, *pieces.shape[1:]))
    gathered = exchanged(pieces.reshape(2 * tp_count, *pieces.shape[2:]), ("c", "tp"))
    starts = [0]
    for weight in mine:
        starts.append(starts[-1] + weight.shape[0])

    side["bundle"] = bundle
    sent_shape = (half, ff_cols + LANES)
    resid_shape = (half, 2 * own_cols)
    sent, side["resid"] = in_kernel(
        entry_kernel,
        (sent_shape, resid_shape),
        gathered.reshape(2 * own_cols, half),
        gain_pre[None, :],
        mine[0],
        mine[1],
        bundle,
    )

    def ff_hidden(sent):
        sent = sent.reshape(z_count, per_z, ff_cols + LANES)
        owned = jnp.sum(exchanged(sent, "z").astype(f32), axis=0)
        total = owned[:, ff_cols : ff_cols + 1] + owned[:, ff_cols + 1 : ff_cols + 2]
        scale = lax.rsqrt(total / D + EPSILON)
        gate = owned[:, :hidden] * scale
        up = owned[:, hidden:ff_cols] * scale
        act = (jax.nn.silu(gate) * up).astype(bf16)
        return sent_to_all(act, "z").reshape(half, hidden)

    partial_shape = (tp_count, *resid_shape)
    act = ff_hidden(sent)
    (partials,) = in_kernel(
        lambda *refs: down_kernel(*refs[:-1], starts[9], refs[-1]),
        (partial_shape,),
        act,
        pre_down,
        side["bundle"],
    )
    summed = jnp.sum(exchanged(partials, "tp").astype(f32), axis=0)
    resid = (side["resid"].astype(f32) + 0.5 * summed).astype(bf16)
    side["resid"] = resid

    turned = jnp.concatenate([resid[:, own_cols:], resid[:, :own_cols]], axis=1)
    swapped = lax.ppermute(turned, "c", swap)
    (sent,) = in_kernel(
        lambda *refs: mix_kernel(*refs[:-1], starts[4], refs[-1]),
        ((packed, 4 * head_cols + LANES),),
        side["spread"],
        resid,
        swapped,
        gain_mix[None, :],
        *mine[4:8],
        side["bundle"],
    )
    sent = sent.reshape(z_count, seq_local * W, 4 * head_cols + LANES)
    side["recur"] = (lengths[None, :], forget_floor[None, :], head_gain[None, :])
    side["states"] = states.reshape(seq_local * heads_local, DK, DK)
    received = exchanged(sent, "z")
    head_out, side["states"] = recurred(received, *side.pop("recur"), side["states"])
    all_heads = sent_to_all(head_out, ("z", "c")).reshape(slot_count, DK)
    partials, new_states = head_partials(
        all_heads,
        side["my_table"],
        mix_weight,
        side.pop("states"),
        side["bundle"],
        starts[8],
        partial_shape,
    )
    sent, side["resid"] = in_kernel(
        lambda *refs: post_kernel(*refs[:-2], starts[2], *refs[-2:]),
        (sent_shape, resid_shape),
        exchanged(partials, "tp"),
        side["resid"],
        gain_post[None, :],
        mine[2],
        mine[3],
        side["bundle"],
    )
    act = ff_hidden(sent)
    (finish,) = in_kernel(
        lambda *refs: finish_kernel(*refs[:-1], starts[10], refs[-1]),
        ((2 * own_cols, half),),
        act,
        side["resid"],
        post_down,
        side["bundle"],
        dtype=f32,
    )
    piece = own_cols // tp_count
    finish = finish.reshape(2 * tp_count, piece * half)
    finished = jnp.sum(exchanged(finish, ("c", "tp")).reshape(2, tp_count, -1), axis=1)
    finished = finished.reshape(2, piece, half)
    finished = jnp.concatenate([finished[0], finished[1]], axis=1).astype(bf16)
    outcome = matmul(finished, side["table"]).astype(bf16).T
    return (outcome, new_states.reshape(states.shape))


def solution(mesh):
    kv = mesh.shape["kv"]
    tp = mesh.shape["tp"]
    cut = Mesh(mesh.devices.reshape(kv // 2, 2, tp), ("z", "c", "tp"))
    kv_axes = ("z", "c")
    placed = (
        P(None, ("z", "c", "tp")),
        P(),
        P(kv_axes, "tp", None, None),
        P(kv_axes),
        P(kv_axes, "tp"),
        P(kv_axes, "tp"),
        P("tp", kv_axes),
        P(kv_axes),
        P(kv_axes, "tp"),
        P(kv_axes, "tp"),
        P(kv_axes, "tp"),
        P(kv_axes, "tp"),
        P("tp"),
        P(),
        P("tp", kv_axes),
        P(kv_axes),
        P(kv_axes, "tp"),
        P(kv_axes, "tp"),
        P("tp", kv_axes),
    )
    return jax.shard_map(
        local,
        mesh=cut,
        in_specs=placed,
        out_specs=(P(None, ("z", "c", "tp")), P(kv_axes, "tp", None, None)),
        check_vma=False,
    )
```

```python
import functools

import jax
import jax.numpy as jnp
from jax import lax
from jax.experimental import pallas as pl
from jax.experimental.pallas import tpu as pltpu
from jax.sharding import Mesh
from jax.sharding import PartitionSpec as P

D = 4096
DK = 128
W = 4
EPSILON = 1e-06
LANES = 128
GAIN_ROWS = 16

f32 = jnp.float32
bf16 = jnp.bfloat16
barrier = lax.optimization_barrier
SMALL = pltpu.CompilerParams(vmem_limit_bytes=16 * 2**20)


def matmul(a, b):
    return jnp.dot(a, b, preferred_element_type=f32)


def in_vmem(value):
    return pltpu.with_memory_space_constraint(value, pltpu.VMEM)


def matmul_t(a, b):
    return lax.dot_general(a, b, (((1,), (1,)), ((), ())), preferred_element_type=f32)


def iota(shape, axis):
    return lax.broadcasted_iota(jnp.int32, shape, axis)


def tables_of(lengths, tokens, core):
    slots = tokens.shape[1]
    packed = slots // 2
    half = packed // 2
    seqs = lengths.shape[1]
    slot = iota((1, slots), 1)
    seq, seq_of = iota((seqs, slots), 0), iota((seqs, slots), 1) // W
    wide = jnp.broadcast_to(lengths, (8, seqs)).astype(bf16)
    before = matmul(wide, (seq < seq_of).astype(f32).astype(bf16))[:1]
    own = matmul(wide, (seq == seq_of).astype(f32).astype(bf16))[:1]
    within = (slot % W).astype(f32)
    targets = jnp.where(within < own, before + within, -1.0)
    rows = iota((packed, slots), 0).astype(f32)
    table = (rows == targets).astype(f32).astype(bf16)
    rows = (iota((half, slots), 0) + core * half).astype(f32)
    my_table = (rows == targets).astype(f32).astype(bf16)
    place = iota((packed, 1), 0)
    my_slot = place // 8 * 16 + core * 8 + place % 8
    before, own = counted(lengths, my_slot)
    within = (my_slot % W).astype(f32)
    targets = jnp.where(within < own, before + within, -1.0)
    row_ids = ((iota((1, packed), 1) + core * half) % packed).astype(f32)
    spread = (targets == row_ids).astype(f32).astype(bf16)
    entry = matmul_t(tokens, table).astype(bf16)
    return table, my_table, spread, entry


def counted(lengths, slots):
    seq = iota((slots.shape[0], lengths.shape[1]), 1)
    before = jnp.sum(jnp.where(seq < slots // W, lengths, 0.0), axis=1, keepdims=True)
    own = jnp.sum(jnp.where(seq == slots // W, lengths, 0.0), axis=1, keepdims=True)
    return before, own


def front_kernel(count, *refs):
    weights, small, refs = refs[:count], refs[count : count + 5], refs[count + 5 :]
    out, table, my_table, spread, entry, sems, *held = refs
    first = []
    for i, (ref, copied) in enumerate(zip(small, held, strict=True)):
        first.append(pltpu.make_async_copy(ref, copied, sems.at[count + i]))
        first[-1].start()
    gains, (lengths, tokens) = held[:3], held[3:]
    copies = []
    at = 0
    for i, ref in enumerate(weights):
        rows = ref.shape[0]
        copies.append(pltpu.make_async_copy(ref, out.at[pl.ds(at, rows)], sems.at[i]))
        copies[-1].start()
        at += rows
    for copy in first:
        copy.wait()
    pieces = []
    for ref in gains:
        value = ref[...]
        high = value.astype(bf16).astype(f32)
        rest = value - high
        mid = rest.astype(bf16).astype(f32)
        pieces += [high, mid, rest - mid]
    pieces.append(jnp.zeros((GAIN_ROWS - len(pieces), LANES), f32))
    out[at:, :] = jnp.concatenate(pieces, axis=0).astype(bf16)
    results = tables_of(lengths[...].astype(f32), tokens[...], lax.axis_index("c"))
    for ref, value in zip((table, my_table, spread, entry), results, strict=True):
        ref[...] = value
    for copy in copies:
        copy.wait()


def front(weights, gains, lengths, tokens):
    rows = sum(w.shape[0] for w in weights) + GAIN_ROWS
    slots = tokens.shape[1]
    packed = slots // 2
    shapes = (
        (rows, weights[0].shape[1]),
        (packed, slots),
        (packed // 2, slots),
        (packed, packed),
        (tokens.shape[0], packed),
    )
    small = (*[gain[None, :] for gain in gains], lengths[None, :], tokens)
    count = len(weights) + len(small)
    return pl.pallas_call(
        functools.partial(front_kernel, len(weights)),
        in_specs=[pl.BlockSpec(memory_space=pl.ANY)] * count,
        out_specs=[pl.BlockSpec(memory_space=pltpu.VMEM)] * len(shapes),
        out_shape=[pltpu.VMEM(shape, bf16) for shape in shapes],
        scratch_shapes=[
            pltpu.SemaphoreType.DMA((count,)),
            *[pltpu.VMEM(value.shape, value.dtype) for value in small],
        ],
    )(*weights, *small)


def recur_kernel(sums, lengths, floors, head_gain, states, heads, new_states):
    total = jnp.sum(sums[...].astype(f32), axis=0)
    at = 4 * DK
    stats = total[:, 2 * at :]
    squares = jnp.concatenate(
        [stats[:, 0:1] + stats[:, 1:2], stats[:, 2:3] + stats[:, 3:4]], axis=0
    )
    total = jnp.concatenate([total[:, :at], total[:, at : 2 * at]], axis=0)
    slots = total.shape[0]
    total = total * lax.rsqrt(squares / D + EPSILON)
    queries = total[:, :DK]
    queries = queries * jax.nn.sigmoid(queries)
    fresh = total[:, 2 * DK : 3 * DK]
    gating = total[:, 3 * DK :]
    first = (lax.axis_index("z") * 2 + lax.axis_index("c")) * slots
    slot = iota((slots, 1), 0) + first
    _, own = counted(lengths[...].astype(f32), slot)
    live = ((slot % W).astype(f32) < own).astype(f32)
    floor = floors[...]
    forgets = floor + (1.0 - floor) * jax.nn.sigmoid(total[:, DK : 2 * DK])
    forgets = jnp.where(live > 0, forgets, 1.0)
    both = jnp.concatenate([queries, forgets], axis=0).T
    readings = []
    for seq in range(states.shape[0]):
        carried = states[seq]
        for offset in range(W):
            row = seq * W + offset
            query = both[:, row : row + 1]
            forget = both[:, slots + row : slots + row + 1]
            carried = forget * carried + (1.0 - forget) * fresh[row : row + 1]
            readings.append(jnp.sum(query * carried, axis=0, keepdims=True))
        new_states[seq] = carried
    read_out = jnp.concatenate(readings, axis=0)
    meansq = jnp.mean(read_out * read_out, axis=1, keepdims=True)
    gate = gating * jax.nn.sigmoid(gating)
    out = read_out * lax.rsqrt(meansq + EPSILON) * head_gain[...] * gate * live
    heads[...] = out.astype(bf16)


def recurred(sums, lengths, floors, head_gain, states):
    vmem = pl.BlockSpec(memory_space=pltpu.VMEM)
    return pl.pallas_call(
        recur_kernel,
        in_specs=[vmem] * 5,
        out_specs=[vmem, vmem],
        out_shape=[pltpu.VMEM((2 * sums.shape[1], DK), bf16), pltpu.VMEM(states.shape, f32)],
        compiler_params=SMALL,
    )(*[in_vmem(value) for value in (sums, lengths, floors, head_gain, states)])


def gain_rows(bundle, which):
    at = bundle.shape[0] - GAIN_ROWS + 3 * which
    return jnp.sum(bundle[at : at + 3, :].astype(f32), axis=0, keepdims=True)


def stats_of(own, other, at):
    total = jnp.sum(own * own + other * other, axis=1, keepdims=True)
    upper = total.astype(bf16).astype(f32)
    lanes = iota((1, LANES), 1)
    return jnp.where(lanes == at, upper, jnp.where(lanes == at + 1, total - upper, 0.0))


def products(own, other, gains, weights, product, exact):
    parts = []
    for rows, gain in zip((own, other), gains, strict=True):
        wide = rows * gain
        whole = wide.astype(bf16)
        if exact:
            rest = (wide - whole.astype(f32)).astype(bf16)
            whole = jnp.concatenate([whole, rest], axis=0)
        parts.append(whole)
    count = own.shape[0]
    results = []
    for ours, theirs in weights:
        both = product(parts[0], ours) + product(parts[1], theirs)
        if exact:
            both = both[:count] + both[count:]
        results.append(both)
    return results


def put_rows(sent, results, stats):
    at = 0
    for result in (*results, stats):
        sent[:, at : at + result.shape[1]] = result.astype(bf16)
        at += result.shape[1]


def put_slots(sent, results, stats):
    groups = sent.shape[0]
    width = sum(result.shape[1] for result in results)
    at = 0
    for result in results:
        cols = result.shape[1]
        slots = result.reshape(groups, 2 * W, cols)
        sent[:, :, at : at + cols] = slots[:, :W].astype(bf16)
        sent[:, :, width + at : width + at + cols] = slots[:, W:].astype(bf16)
        at += cols
    low, high = [value.reshape(groups, 2 * W, LANES) for value in stats]
    sent[:, :, 2 * width :] = (low[:, :W] + high[:, W:]).astype(bf16)


def halves_of(weights, bundle, at):
    pairs = []
    for weight in weights:
        pairs.append((weight[...], bundle[at : at + weight.shape[0], :]))
        at += weight.shape[0]
    return pairs


def entry_kernel(gathered, gain, gate, up, bundle, sent, resid):
    cols = gain.shape[1]
    first = lax.axis_index("c") == 0
    low, high = gathered[:cols, :].astype(f32), gathered[cols:, :].astype(f32)
    own = jnp.where(first, low, high).T
    other = jnp.where(first, high, low).T
    resid[:, :cols] = own.astype(bf16)
    resid[:, cols:] = other.astype(bf16)
    weights = halves_of((gate, up), bundle, 0)
    gains = (gain[...], gain_rows(bundle, 0))
    results = products(own, other, gains, weights, matmul_t, True)
    put_rows(sent, results, stats_of(own, other, 0))


def mix_kernel(spread, resid, swapped, gain, query, forget, value, outgate, bundle, at, sent):
    cols = gain.shape[1]
    rows = jnp.concatenate([resid[...], swapped[...]], axis=0)
    rows = matmul(spread[...], rows)
    weights = halves_of((query, forget, value, outgate), bundle, at)
    gains = (gain[...], gain_rows(bundle, 1))
    own, other = rows[:, :cols], rows[:, cols:]
    results = products(own, other, gains, weights, matmul, True)
    put_slots(sent, results, (stats_of(own, other, 0), stats_of(own, other, 2)))


def post_kernel(received, before, gain, gate, up, bundle, at, sent, resid):
    cols = gain.shape[1]
    total = jnp.sum(received[...].astype(f32), axis=0)
    rows = (before[...].astype(f32) + total).astype(bf16)
    resid[...] = rows
    rows = rows.astype(f32)
    weights = halves_of((gate, up), bundle, at)
    gains = (gain[...], gain_rows(bundle, 2))
    own, other = rows[:, :cols], rows[:, cols:]
    results = products(own, other, gains, weights, matmul_t, False)
    put_rows(sent, results, stats_of(own, other, 0))


def put_partials(rows, weight, other, out):
    cols = weight.shape[1]
    own = matmul(rows, weight[...]).astype(bf16)
    other = matmul(rows, other).astype(bf16)
    for i in range(out.shape[0]):
        out[i, :, :cols] = own
        out[i, :, cols:] = other


def down_kernel(rows, weight, bundle, at, out):
    put_partials(rows[...], weight, bundle[at : at + weight.shape[0], :], out)


def heads_kernel(heads, table, weight, states, bundle, at, out, new_states, sem):
    copy = pltpu.make_async_copy(states, new_states, sem)
    copy.start()
    rows = matmul(table[...], heads[...]).astype(bf16)
    put_partials(rows, weight, bundle[at : at + weight.shape[0], :], out)
    copy.wait()


def head_partials(heads, table, weight, states, bundle, at, shape):
    vmem = pl.BlockSpec(memory_space=pltpu.VMEM)
    values = [in_vmem(value) for value in (heads, table, weight, states, bundle)]
    return pl.pallas_call(
        lambda *refs: heads_kernel(*refs[:5], at, *refs[5:]),
        in_specs=[vmem] * len(values),
        out_specs=[vmem, pl.BlockSpec(memory_space=pl.ANY)],
        out_shape=[pltpu.VMEM(shape, bf16), jax.ShapeDtypeStruct(states.shape, f32)],
        scratch_shapes=[pltpu.SemaphoreType.DMA],
        compiler_params=SMALL,
    )(*values)


def finish_kernel(rows, resid, weight, bundle, at, out):
    cols = weight.shape[1]
    first = (lax.axis_index("tp") == 0).astype(f32)
    own = 0.5 * matmul(rows[...], weight[...]) + first * resid[:, :cols].astype(f32)
    other = matmul(rows[...], bundle[at : at + weight.shape[0], :])
    other = 0.5 * other + first * resid[:, cols:].astype(f32)
    own, other = own.T, other.T
    leads = lax.axis_index("c") == 0
    out[:cols, :] = jnp.where(leads, own, other)
    out[cols:, :] = jnp.where(leads, other, own)


def last_kernel(received, table, out):
    groups, size = received.shape
    half = table.shape[0] // 2
    low = jnp.sum(received[: groups // 2, :], axis=0, keepdims=True)
    high = jnp.sum(received[groups // 2 :, :], axis=0, keepdims=True)
    rows = [
        jnp.concatenate([low[:, at : at + half], high[:, at : at + half]], axis=1)
        for at in range(0, size, half)
    ]
    out[...] = matmul(jnp.concatenate(rows, axis=0).astype(bf16), table[...]).astype(bf16)


def last_spread(received, table, cols):
    vmem = pl.BlockSpec(memory_space=pltpu.VMEM)
    return pl.pallas_call(
        last_kernel,
        in_specs=[vmem, vmem],
        out_specs=vmem,
        out_shape=jax.ShapeDtypeStruct((cols, table.shape[1]), bf16),
        compiler_params=SMALL,
    )(in_vmem(received), in_vmem(table))


def in_kernel(kernel, shapes, *values, dtype=bf16):
    vmem = pl.BlockSpec(memory_space=pltpu.VMEM)
    return pl.pallas_call(
        kernel,
        in_specs=[vmem] * len(values),
        out_specs=[vmem] * len(shapes),
        out_shape=[pltpu.VMEM(shape, dtype) for shape in shapes],
        compiler_params=SMALL,
    )(*[in_vmem(value) for value in values])


def local(
    tokens,
    lengths,
    states,
    gain_pre,
    pre_gate,
    pre_up,
    pre_down,
    gain_mix,
    query_weight,
    forget_weight,
    input_weight,
    outgate_weight,
    forget_floor,
    head_gain,
    mix_weight,
    gain_post,
    post_gate,
    post_up,
    post_down,
):
    z_count = lax.axis_size("z")
    tp_count = lax.axis_size("tp")
    slot_count = tokens.shape[0]
    packed = slot_count // 2
    half = packed // 2
    per_z = half // z_count
    own_cols = gain_pre.shape[0]
    hidden = pre_gate.shape[1]
    ff_cols = 2 * hidden
    head_cols = query_weight.shape[1]
    seq_local, heads_local = states.shape[:2]
    swap = [(0, 1), (1, 0)]

    side = {}

    def exchanged(value, axis):
        value, tied = barrier((value, dict(side)))
        value = lax.all_to_all(value, axis, split_axis=0, concat_axis=0, tiled=True)
        value, tied = barrier((value, tied))
        side.update(tied)
        return value

    def sent_to_all(value, axis):
        return exchanged(jnp.broadcast_to(value, (lax.axis_size(axis), *value.shape)), axis)

    mine = (pre_gate.T, pre_up.T, post_gate.T, post_up.T)
    mine += (query_weight, forget_weight, input_weight, outgate_weight)
    mine += (mix_weight, pre_down, post_down)
    gains = (gain_pre, gain_mix, gain_post)
    packed_own, table, my_table, spread, entry = front(mine, gains, lengths, tokens.T)
    bundle = lax.ppermute(packed_own, "c", swap)

    side["table"] = table
    side["my_table"] = my_table
    side["spread"] = spread

    pieces = jnp.stack([entry[:, :half], entry[:, half:]])
    pieces = jnp.broadcast_to(pieces[:, None], (2, tp_count, *pieces.shape[1:]))
    gathered = exchanged(pieces.reshape(2 * tp_count, *pieces.shape[2:]), ("c", "tp"))
    starts = [0]
    for weight in mine:
        starts.append(starts[-1] + weight.shape[0])

    side["bundle"] = bundle
    sent_shape = (half, ff_cols + LANES)
    resid_shape = (half, 2 * own_cols)
    sent, side["resid"] = in_kernel(
        entry_kernel,
        (sent_shape, resid_shape),
        gathered.reshape(2 * own_cols, half),
        gain_pre[None, :],
        mine[0],
        mine[1],
        bundle,
    )

    def ff_hidden(sent):
        sent = sent.reshape(z_count, per_z, ff_cols + LANES)
        owned = jnp.sum(exchanged(sent, "z").astype(f32), axis=0)
        total = owned[:, ff_cols : ff_cols + 1] + owned[:, ff_cols + 1 : ff_cols + 2]
        scale = lax.rsqrt(total / D + EPSILON)
        gate = owned[:, :hidden] * scale
        up = owned[:, hidden:ff_cols] * scale
        act = (jax.nn.silu(gate) * up).astype(bf16)
        return sent_to_all(act, "z").reshape(half, hidden)

    partial_shape = (tp_count, *resid_shape)
    act = ff_hidden(sent)
    (partials,) = in_kernel(
        lambda *refs: down_kernel(*refs[:-1], starts[9], refs[-1]),
        (partial_shape,),
        act,
        pre_down,
        side["bundle"],
    )
    summed = jnp.sum(exchanged(partials, "tp").astype(f32), axis=0)
    resid = (side["resid"].astype(f32) + 0.5 * summed).astype(bf16)
    side["resid"] = resid

    turned = jnp.concatenate([resid[:, own_cols:], resid[:, :own_cols]], axis=1)
    swapped = lax.ppermute(turned, "c", swap)
    (sent,) = in_kernel(
        lambda *refs: mix_kernel(*refs[:-1], starts[4], refs[-1]),
        ((z_count, W, 8 * head_cols + LANES),),
        side["spread"],
        resid,
        swapped,
        gain_mix[None, :],
        *mine[4:8],
        side["bundle"],
    )
    side["recur"] = (lengths[None, :], forget_floor[None, :], head_gain[None, :])
    side["states"] = states.reshape(seq_local * heads_local, DK, DK)
    received = exchanged(sent, "z")
    head_out, side["states"] = recurred(received, *side.pop("recur"), side["states"])
    all_heads = sent_to_all(head_out, ("z", "c")).reshape(slot_count, DK)
    partials, new_states = head_partials(
        all_heads,
        side["my_table"],
        mix_weight,
        side.pop("states"),
        side["bundle"],
        starts[8],
        partial_shape,
    )
    sent, side["resid"] = in_kernel(
        lambda *refs: post_kernel(*refs[:-2], starts[2], *refs[-2:]),
        (sent_shape, resid_shape),
        exchanged(partials, "tp"),
        side["resid"],
        gain_post[None, :],
        mine[2],
        mine[3],
        side["bundle"],
    )
    act = ff_hidden(sent)
    (finish,) = in_kernel(
        lambda *refs: finish_kernel(*refs[:-1], starts[10], refs[-1]),
        ((2 * own_cols, half),),
        act,
        side["resid"],
        post_down,
        side["bundle"],
        dtype=f32,
    )
    piece = own_cols // tp_count
    finish = finish.reshape(2 * tp_count, piece * half)
    outcome = last_spread(exchanged(finish, ("c", "tp")), side["table"], piece).T
    return (outcome, new_states.reshape(states.shape))


def solution(mesh):
    kv = mesh.shape["kv"]
    tp = mesh.shape["tp"]
    cut = Mesh(mesh.devices.reshape(kv // 2, 2, tp), ("z", "c", "tp"))
    kv_axes = ("z", "c")
    placed = (
        P(None, ("z", "c", "tp")),
        P(),
        P(kv_axes, "tp", None, None),
        P(kv_axes),
        P(kv_axes, "tp"),
        P(kv_axes, "tp"),
        P("tp", kv_axes),
        P(kv_axes),
        P(kv_axes, "tp"),
        P(kv_axes, "tp"),
        P(kv_axes, "tp"),
        P(kv_axes, "tp"),
        P("tp"),
        P(),
        P("tp", kv_axes),
        P(kv_axes),
        P(kv_axes, "tp"),
        P(kv_axes, "tp"),
        P("tp", kv_axes),
    )
    return jax.shard_map(
        local,
        mesh=cut,
        in_specs=placed,
        out_specs=(P(None, ("z", "c", "tp")), P(kv_axes, "tp", None, None)),
        check_vma=False,
    )
```

```python
import functools

import jax
import jax.numpy as jnp
from jax import lax
from jax.experimental import pallas as pl
from jax.experimental.pallas import tpu as pltpu
from jax.sharding import Mesh
from jax.sharding import PartitionSpec as P

D = 4096
DK = 128
W = 4
EPSILON = 1e-06
LANES = 128
GAIN_ROWS = 16

f32 = jnp.float32
bf16 = jnp.bfloat16
barrier = lax.optimization_barrier
SMALL = pltpu.CompilerParams(vmem_limit_bytes=16 * 2**20)


def matmul(a, b):
    return jnp.dot(a, b, preferred_element_type=f32)


def in_vmem(value):
    return pltpu.with_memory_space_constraint(value, pltpu.VMEM)


def matmul_t(a, b):
    return lax.dot_general(a, b, (((1,), (1,)), ((), ())), preferred_element_type=f32)


def iota(shape, axis):
    return lax.broadcasted_iota(jnp.int32, shape, axis)


def tables_of(lengths, tokens, core):
    slots = tokens.shape[1]
    packed = slots // 2
    half = packed // 2
    seqs = lengths.shape[1]
    slot = iota((1, slots), 1)
    seq, seq_of = iota((seqs, slots), 0), iota((seqs, slots), 1) // W
    wide = jnp.broadcast_to(lengths, (8, seqs)).astype(bf16)
    before = matmul(wide, (seq < seq_of).astype(f32).astype(bf16))[:1]
    own = matmul(wide, (seq == seq_of).astype(f32).astype(bf16))[:1]
    within = (slot % W).astype(f32)
    targets = jnp.where(within < own, before + within, -1.0)
    rows = iota((packed, slots), 0).astype(f32)
    table = (rows == targets).astype(f32).astype(bf16)
    rows = (iota((half, slots), 0) + core * half).astype(f32)
    my_table = (rows == targets).astype(f32).astype(bf16)
    place = iota((packed, 1), 0)
    my_slot = place // 8 * 16 + core * 8 + place % 8
    before, own = counted(lengths, my_slot)
    within = (my_slot % W).astype(f32)
    targets = jnp.where(within < own, before + within, -1.0)
    row_ids = ((iota((1, packed), 1) + core * half) % packed).astype(f32)
    spread = (targets == row_ids).astype(f32).astype(bf16)
    entry = matmul_t(tokens, table)
    cols = entry.shape[0] // 2
    entry = jnp.stack(
        [
            jnp.concatenate([entry[:cols, at : at + half], entry[cols:, at : at + half]], axis=1)
            for at in (0, half)
        ]
    ).astype(bf16)
    return table, my_table, spread, entry


def counted(lengths, slots):
    seq = iota((slots.shape[0], lengths.shape[1]), 1)
    before = jnp.sum(jnp.where(seq < slots // W, lengths, 0.0), axis=1, keepdims=True)
    own = jnp.sum(jnp.where(seq == slots // W, lengths, 0.0), axis=1, keepdims=True)
    return before, own


def front_kernel(count, *refs):
    weights, small, refs = refs[:count], refs[count : count + 5], refs[count + 5 :]
    out, table, my_table, spread, entry, sems, *held = refs
    first = []
    for i, (ref, copied) in enumerate(zip(small, held, strict=True)):
        first.append(pltpu.make_async_copy(ref, copied, sems.at[count + i]))
        first[-1].start()
    gains, (lengths, tokens) = held[:3], held[3:]
    copies = []
    at = 0
    for i, ref in enumerate(weights):
        rows = ref.shape[0]
        copies.append(pltpu.make_async_copy(ref, out.at[pl.ds(at, rows)], sems.at[i]))
        copies[-1].start()
        at += rows
    for copy in first:
        copy.wait()
    pieces = []
    for ref in gains:
        value = ref[...]
        high = value.astype(bf16).astype(f32)
        rest = value - high
        mid = rest.astype(bf16).astype(f32)
        pieces += [high, mid, rest - mid]
    pieces.append(jnp.zeros((GAIN_ROWS - len(pieces), LANES), f32))
    out[at:, :] = jnp.concatenate(pieces, axis=0).astype(bf16)
    results = tables_of(lengths[...].astype(f32), tokens[...], lax.axis_index("c"))
    for ref, value in zip((table, my_table, spread, entry), results, strict=True):
        ref[...] = value
    for copy in copies:
        copy.wait()


def front(weights, gains, lengths, tokens):
    rows = sum(w.shape[0] for w in weights) + GAIN_ROWS
    slots = tokens.shape[1]
    packed = slots // 2
    shapes = (
        (rows, weights[0].shape[1]),
        (packed, slots),
        (packed // 2, slots),
        (packed, packed),
        (2, tokens.shape[0] // 2, packed),
    )
    small = (*[gain[None, :] for gain in gains], lengths[None, :], tokens)
    count = len(weights) + len(small)
    return pl.pallas_call(
        functools.partial(front_kernel, len(weights)),
        in_specs=[pl.BlockSpec(memory_space=pl.ANY)] * count,
        out_specs=[pl.BlockSpec(memory_space=pltpu.VMEM)] * len(shapes),
        out_shape=[pltpu.VMEM(shape, bf16) for shape in shapes],
        scratch_shapes=[
            pltpu.SemaphoreType.DMA((count,)),
            *[pltpu.VMEM(value.shape, value.dtype) for value in small],
        ],
    )(*weights, *small)


def recur_kernel(sums, lengths, floors, head_gain, states, heads, new_states):
    total = jnp.sum(sums[...].astype(f32), axis=0)
    at = 4 * DK
    stats = total[:, 2 * at :]
    squares = jnp.concatenate(
        [stats[:, 0:1] + stats[:, 1:2], stats[:, 2:3] + stats[:, 3:4]], axis=0
    )
    total = jnp.concatenate([total[:, :at], total[:, at : 2 * at]], axis=0)
    slots = total.shape[0]
    total = total * lax.rsqrt(squares / D + EPSILON)
    queries = total[:, :DK]
    queries = queries * jax.nn.sigmoid(queries)
    fresh = total[:, 2 * DK : 3 * DK]
    gating = total[:, 3 * DK :]
    first = (lax.axis_index("z") * 2 + lax.axis_index("c")) * slots
    slot = iota((slots, 1), 0) + first
    _, own = counted(lengths[...].astype(f32), slot)
    live = ((slot % W).astype(f32) < own).astype(f32)
    floor = floors[...]
    forgets = floor + (1.0 - floor) * jax.nn.sigmoid(total[:, DK : 2 * DK])
    forgets = jnp.where(live > 0, forgets, 1.0)
    both = jnp.concatenate([queries, forgets], axis=0).T
    readings = []
    for seq in range(states.shape[0]):
        carried = states[seq]
        for offset in range(W):
            row = seq * W + offset
            query = both[:, row : row + 1]
            forget = both[:, slots + row : slots + row + 1]
            carried = forget * carried + (1.0 - forget) * fresh[row : row + 1]
            readings.append(jnp.sum(query * carried, axis=0, keepdims=True))
        new_states[seq] = carried
    read_out = jnp.concatenate(readings, axis=0)
    meansq = jnp.mean(read_out * read_out, axis=1, keepdims=True)
    gate = gating * jax.nn.sigmoid(gating)
    out = read_out * lax.rsqrt(meansq + EPSILON) * head_gain[...] * gate * live
    heads[...] = out.astype(bf16)


def recurred(sums, lengths, floors, head_gain, states):
    vmem = pl.BlockSpec(memory_space=pltpu.VMEM)
    return pl.pallas_call(
        recur_kernel,
        in_specs=[vmem] * 5,
        out_specs=[vmem, vmem],
        out_shape=[pltpu.VMEM((2 * sums.shape[1], DK), bf16), pltpu.VMEM(states.shape, f32)],
        compiler_params=SMALL,
    )(*[in_vmem(value) for value in (sums, lengths, floors, head_gain, states)])


def gain_rows(bundle, which):
    at = bundle.shape[0] - GAIN_ROWS + 3 * which
    return jnp.sum(bundle[at : at + 3, :].astype(f32), axis=0, keepdims=True)


def stats_of(own, other, at):
    total = jnp.sum(own * own + other * other, axis=1, keepdims=True)
    upper = total.astype(bf16).astype(f32)
    lanes = iota((1, LANES), 1)
    return jnp.where(lanes == at, upper, jnp.where(lanes == at + 1, total - upper, 0.0))


def products(own, other, gains, weights, product, exact):
    parts = []
    for rows, gain in zip((own, other), gains, strict=True):
        wide = rows * gain
        whole = wide.astype(bf16)
        if exact:
            rest = (wide - whole.astype(f32)).astype(bf16)
            whole = jnp.concatenate([whole, rest], axis=0)
        parts.append(whole)
    count = own.shape[0]
    results = []
    for ours, theirs in weights:
        both = product(parts[0], ours) + product(parts[1], theirs)
        if exact:
            both = both[:count] + both[count:]
        results.append(both)
    return results


def put_rows(sent, results, stats):
    at = 0
    for result in (*results, stats):
        sent[:, at : at + result.shape[1]] = result.astype(bf16)
        at += result.shape[1]


def put_slots(sent, results, stats):
    groups = sent.shape[0]
    width = sum(result.shape[1] for result in results)
    at = 0
    for result in results:
        cols = result.shape[1]
        slots = result.reshape(groups, 2 * W, cols)
        sent[:, :, at : at + cols] = slots[:, :W].astype(bf16)
        sent[:, :, width + at : width + at + cols] = slots[:, W:].astype(bf16)
        at += cols
    low, high = [value.reshape(groups, 2 * W, LANES) for value in stats]
    sent[:, :, 2 * width :] = (low[:, :W] + high[:, W:]).astype(bf16)


def halves_of(weights, bundle, at):
    pairs = []
    for weight in weights:
        pairs.append((weight[...], bundle[at : at + weight.shape[0], :]))
        at += weight.shape[0]
    return pairs


def entry_kernel(gathered, gain, gate, up, bundle, sent, resid):
    cols = gain.shape[1]
    first = lax.axis_index("c") == 0
    groups = gathered.shape[0] // 2
    halves = []
    for at in (0, groups):
        pairs = gathered[at : at + groups].astype(f32)
        rows = pairs.shape[2] // 2
        pairs = jnp.concatenate([pairs[:, :, :rows], pairs[:, :, rows:]], axis=1)
        halves.append(pairs.reshape(cols, rows))
    low, high = halves
    own = jnp.where(first, low, high).T
    other = jnp.where(first, high, low).T
    resid[:, :cols] = own.astype(bf16)
    resid[:, cols:] = other.astype(bf16)
    weights = halves_of((gate, up), bundle, 0)
    gains = (gain[...], gain_rows(bundle, 0))
    results = products(own, other, gains, weights, matmul_t, True)
    put_rows(sent, results, stats_of(own, other, 0))


def mix_kernel(spread, resid, swapped, gain, query, forget, value, outgate, bundle, at, sent):
    cols = gain.shape[1]
    rows = jnp.concatenate([resid[...], swapped[...]], axis=0)
    rows = matmul(spread[...], rows)
    weights = halves_of((query, forget, value, outgate), bundle, at)
    gains = (gain[...], gain_rows(bundle, 1))
    own, other = rows[:, :cols], rows[:, cols:]
    results = products(own, other, gains, weights, matmul, True)
    put_slots(sent, results, (stats_of(own, other, 0), stats_of(own, other, 2)))


def post_kernel(received, before, gain, gate, up, bundle, at, sent, resid):
    cols = gain.shape[1]
    total = jnp.sum(received[...].astype(f32), axis=0)
    rows = (before[...].astype(f32) + total).astype(bf16)
    resid[...] = rows
    rows = rows.astype(f32)
    weights = halves_of((gate, up), bundle, at)
    gains = (gain[...], gain_rows(bundle, 2))
    own, other = rows[:, :cols], rows[:, cols:]
    results = products(own, other, gains, weights, matmul_t, False)
    put_rows(sent, results, stats_of(own, other, 0))


def put_partials(rows, weight, other, out):
    cols = weight.shape[1]
    own = matmul(rows, weight[...]).astype(bf16)
    other = matmul(rows, other).astype(bf16)
    for i in range(out.shape[0]):
        out[i, :, :cols] = own
        out[i, :, cols:] = other


def hidden_kernel(received, out):
    total = jnp.sum(received[...].astype(f32), axis=0)
    hidden = out.shape[2]
    at = 2 * hidden
    squares = total[:, at : at + 1] + total[:, at + 1 : at + 2]
    scale = lax.rsqrt(squares / D + EPSILON)
    gate = total[:, :hidden] * scale
    up = total[:, hidden:at] * scale
    act = (gate * jax.nn.sigmoid(gate) * up).astype(bf16)
    for i in range(out.shape[0]):
        out[i] = act


def down_kernel(rows, weight, bundle, at, out):
    put_partials(rows[...], weight, bundle[at : at + weight.shape[0], :], out)


def heads_kernel(heads, table, weight, states, bundle, at, out, new_states, sem):
    copy = pltpu.make_async_copy(states, new_states, sem)
    copy.start()
    rows = matmul(table[...], heads[...]).astype(bf16)
    put_partials(rows, weight, bundle[at : at + weight.shape[0], :], out)
    copy.wait()


def head_partials(heads, table, weight, states, bundle, at, shape):
    vmem = pl.BlockSpec(memory_space=pltpu.VMEM)
    values = [in_vmem(value) for value in (heads, table, weight, states, bundle)]
    return pl.pallas_call(
        lambda *refs: heads_kernel(*refs[:5], at, *refs[5:]),
        in_specs=[vmem] * len(values),
        out_specs=[vmem, pl.BlockSpec(memory_space=pl.ANY)],
        out_shape=[pltpu.VMEM(shape, bf16), jax.ShapeDtypeStruct(states.shape, f32)],
        scratch_shapes=[pltpu.SemaphoreType.DMA],
        compiler_params=SMALL,
    )(*values)


def put_pairs(out, at, cols, groups):
    count, rows = cols.shape
    pairs = cols.reshape(groups, count // groups, rows)
    half = count // groups // 2
    paired = jnp.concatenate([pairs[:, :half], pairs[:, half:]], axis=2)
    out[at : at + groups] = paired.astype(out.dtype)


def finish_kernel(rows, resid, weight, bundle, at, out):
    cols = weight.shape[1]
    first = (lax.axis_index("tp") == 0).astype(f32)
    own = 0.5 * matmul(rows[...], weight[...]) + first * resid[:, :cols].astype(f32)
    other = matmul(rows[...], bundle[at : at + weight.shape[0], :])
    other = 0.5 * other + first * resid[:, cols:].astype(f32)
    own, other = own.T, other.T
    leads = lax.axis_index("c") == 0
    groups = out.shape[0] // 2
    put_pairs(out, 0, jnp.where(leads, own, other), groups)
    put_pairs(out, groups, jnp.where(leads, other, own), groups)


def last_kernel(received, table, out):
    groups = received.shape[0] // 2
    half = table.shape[0] // 2
    low = jnp.sum(received[:groups], axis=0)
    high = jnp.sum(received[groups:], axis=0)
    rows = [
        jnp.concatenate([low[:, at : at + half], high[:, at : at + half]], axis=1)
        for at in (0, half)
    ]
    out[...] = matmul(jnp.concatenate(rows, axis=0).astype(bf16), table[...]).astype(bf16)


def last_spread(received, table, cols):
    vmem = pl.BlockSpec(memory_space=pltpu.VMEM)
    return pl.pallas_call(
        last_kernel,
        in_specs=[vmem, vmem],
        out_specs=vmem,
        out_shape=jax.ShapeDtypeStruct((cols, table.shape[1]), bf16),
        compiler_params=SMALL,
    )(in_vmem(received), in_vmem(table))


def in_kernel(kernel, shapes, *values, dtype=bf16):
    vmem = pl.BlockSpec(memory_space=pltpu.VMEM)
    return pl.pallas_call(
        kernel,
        in_specs=[vmem] * len(values),
        out_specs=[vmem] * len(shapes),
        out_shape=[pltpu.VMEM(shape, dtype) for shape in shapes],
        compiler_params=SMALL,
    )(*[in_vmem(value) for value in values])


def local(
    tokens,
    lengths,
    states,
    gain_pre,
    pre_gate,
    pre_up,
    pre_down,
    gain_mix,
    query_weight,
    forget_weight,
    input_weight,
    outgate_weight,
    forget_floor,
    head_gain,
    mix_weight,
    gain_post,
    post_gate,
    post_up,
    post_down,
):
    z_count = lax.axis_size("z")
    tp_count = lax.axis_size("tp")
    slot_count = tokens.shape[0]
    packed = slot_count // 2
    half = packed // 2
    per_z = half // z_count
    own_cols = gain_pre.shape[0]
    hidden = pre_gate.shape[1]
    ff_cols = 2 * hidden
    head_cols = query_weight.shape[1]
    seq_local, heads_local = states.shape[:2]
    swap = [(0, 1), (1, 0)]

    side = {}

    def exchanged(value, axis):
        value, tied = barrier((value, dict(side)))
        value = lax.all_to_all(value, axis, split_axis=0, concat_axis=0, tiled=True)
        value, tied = barrier((value, tied))
        side.update(tied)
        return value

    def sent_to_all(value, axis):
        return exchanged(jnp.broadcast_to(value, (lax.axis_size(axis), *value.shape)), axis)

    mine = (pre_gate.T, pre_up.T, post_gate.T, post_up.T)
    mine += (query_weight, forget_weight, input_weight, outgate_weight)
    mine += (mix_weight, pre_down, post_down)
    gains = (gain_pre, gain_mix, gain_post)
    packed_own, table, my_table, spread, entry = front(mine, gains, lengths, tokens.T)
    bundle = lax.ppermute(packed_own, "c", swap)

    side["table"] = table
    side["my_table"] = my_table
    side["spread"] = spread

    pieces = jnp.broadcast_to(entry[:, None], (2, tp_count, *entry.shape[1:]))
    gathered = exchanged(pieces.reshape(2 * tp_count, *entry.shape[1:]), ("c", "tp"))
    starts = [0]
    for weight in mine:
        starts.append(starts[-1] + weight.shape[0])

    side["bundle"] = bundle
    sent_shape = (half, ff_cols + LANES)
    resid_shape = (half, 2 * own_cols)
    sent, side["resid"] = in_kernel(
        entry_kernel,
        (sent_shape, resid_shape),
        gathered,
        gain_pre[None, :],
        mine[0],
        mine[1],
        bundle,
    )

    def ff_hidden(sent):
        sent = sent.reshape(z_count, per_z, ff_cols + LANES)
        (acts,) = in_kernel(
            hidden_kernel, ((z_count, per_z, hidden),), exchanged(sent, "z")
        )
        return exchanged(acts, "z").reshape(half, hidden)

    partial_shape = (tp_count, *resid_shape)
    act = ff_hidden(sent)
    (partials,) = in_kernel(
        lambda *refs: down_kernel(*refs[:-1], starts[9], refs[-1]),
        (partial_shape,),
        act,
        pre_down,
        side["bundle"],
    )
    summed = jnp.sum(exchanged(partials, "tp").astype(f32), axis=0)
    resid = (side["resid"].astype(f32) + 0.5 * summed).astype(bf16)
    side["resid"] = resid

    turned = jnp.concatenate([resid[:, own_cols:], resid[:, :own_cols]], axis=1)
    swapped = lax.ppermute(turned, "c", swap)
    (sent,) = in_kernel(
        lambda *refs: mix_kernel(*refs[:-1], starts[4], refs[-1]),
        ((z_count, W, 8 * head_cols + LANES),),
        side["spread"],
        resid,
        swapped,
        gain_mix[None, :],
        *mine[4:8],
        side["bundle"],
    )
    side["recur"] = (lengths[None, :], forget_floor[None, :], head_gain[None, :])
    side["states"] = states.reshape(seq_local * heads_local, DK, DK)
    received = exchanged(sent, "z")
    head_out, side["states"] = recurred(received, *side.pop("recur"), side["states"])
    all_heads = sent_to_all(head_out, ("z", "c")).reshape(slot_count, DK)
    partials, new_states = head_partials(
        all_heads,
        side["my_table"],
        mix_weight,
        side.pop("states"),
        side["bundle"],
        starts[8],
        partial_shape,
    )
    sent, side["resid"] = in_kernel(
        lambda *refs: post_kernel(*refs[:-2], starts[2], *refs[-2:]),
        (sent_shape, resid_shape),
        exchanged(partials, "tp"),
        side["resid"],
        gain_post[None, :],
        mine[2],
        mine[3],
        side["bundle"],
    )
    act = ff_hidden(sent)
    (finish,) = in_kernel(
        lambda *refs: finish_kernel(*refs[:-1], starts[10], refs[-1]),
        ((2 * tp_count, own_cols // tp_count // 2, 2 * half),),
        act,
        side["resid"],
        post_down,
        side["bundle"],
        dtype=f32,
    )
    piece = own_cols // tp_count
    outcome = last_spread(exchanged(finish, ("c", "tp")), side["table"], piece).T
    return (outcome, new_states.reshape(states.shape))


def solution(mesh):
    kv = mesh.shape["kv"]
    tp = mesh.shape["tp"]
    cut = Mesh(mesh.devices.reshape(kv // 2, 2, tp), ("z", "c", "tp"))
    kv_axes = ("z", "c")
    placed = (
        P(None, ("z", "c", "tp")),
        P(),
        P(kv_axes, "tp", None, None),
        P(kv_axes),
        P(kv_axes, "tp"),
        P(kv_axes, "tp"),
        P("tp", kv_axes),
        P(kv_axes),
        P(kv_axes, "tp"),
        P(kv_axes, "tp"),
        P(kv_axes, "tp"),
        P(kv_axes, "tp"),
        P("tp"),
        P(),
        P("tp", kv_axes),
        P(kv_axes),
        P(kv_axes, "tp"),
        P(kv_axes, "tp"),
        P("tp", kv_axes),
    )
    return jax.shard_map(
        local,
        mesh=cut,
        in_specs=placed,
        out_specs=(P(None, ("z", "c", "tp")), P(kv_axes, "tp", None, None)),
        check_vma=False,
    )
```

```python
import functools

import jax
import jax.numpy as jnp
from jax import lax
from jax.experimental import pallas as pl
from jax.experimental.pallas import tpu as pltpu
from jax.sharding import Mesh
from jax.sharding import PartitionSpec as P

D = 4096
DK = 128
W = 4
EPSILON = 1e-06
LANES = 128
GAIN_ROWS = 16

f32 = jnp.float32
bf16 = jnp.bfloat16
barrier = lax.optimization_barrier
SMALL = pltpu.CompilerParams(vmem_limit_bytes=16 * 2**20)


def matmul(a, b):
    return jnp.dot(a, b, preferred_element_type=f32)


def in_vmem(value):
    return pltpu.with_memory_space_constraint(value, pltpu.VMEM)


def matmul_t(a, b):
    return lax.dot_general(a, b, (((1,), (1,)), ((), ())), preferred_element_type=f32)


def iota(shape, axis):
    return lax.broadcasted_iota(jnp.int32, shape, axis)


def tables_of(lengths, tokens, core):
    slots = tokens.shape[1]
    packed = slots // 2
    half = packed // 2
    seqs = lengths.shape[1]
    slot = iota((1, slots), 1)
    seq, seq_of = iota((seqs, slots), 0), iota((seqs, slots), 1) // W
    wide = jnp.broadcast_to(lengths, (8, seqs)).astype(bf16)
    before = matmul(wide, (seq < seq_of).astype(f32).astype(bf16))[:1]
    own = matmul(wide, (seq == seq_of).astype(f32).astype(bf16))[:1]
    within = (slot % W).astype(f32)
    targets = jnp.where(within < own, before + within, -1.0)
    rows = iota((packed, slots), 0).astype(f32)
    table = (rows == targets).astype(f32).astype(bf16)
    rows = (iota((half, slots), 0) + core * half).astype(f32)
    my_table = (rows == targets).astype(f32).astype(bf16)
    place = iota((packed, 1), 0)
    my_slot = place // 8 * 16 + core * 8 + place % 8
    before, own = counted(lengths, my_slot)
    within = (my_slot % W).astype(f32)
    targets = jnp.where(within < own, before + within, -1.0)
    row_ids = ((iota((1, packed), 1) + core * half) % packed).astype(f32)
    spread = (targets == row_ids).astype(f32).astype(bf16)
    entry = matmul_t(tokens, table)
    cols = entry.shape[0] // 2
    entry = jnp.stack(
        [
            jnp.concatenate([entry[:cols, at : at + half], entry[cols:, at : at + half]], axis=1)
            for at in (0, half)
        ]
    ).astype(bf16)
    return table, my_table, spread, entry


def counted(lengths, slots):
    seq = iota((slots.shape[0], lengths.shape[1]), 1)
    before = jnp.sum(jnp.where(seq < slots // W, lengths, 0.0), axis=1, keepdims=True)
    own = jnp.sum(jnp.where(seq == slots // W, lengths, 0.0), axis=1, keepdims=True)
    return before, own


def front_kernel(count, *refs):
    weights, small, refs = refs[:count], refs[count : count + 5], refs[count + 5 :]
    out, table, my_table, spread, entry, sems, *held = refs
    first = []
    for i, (ref, copied) in enumerate(zip(small, held, strict=True)):
        first.append(pltpu.make_async_copy(ref, copied, sems.at[count + i]))
        first[-1].start()
    gains, (lengths, tokens) = held[:3], held[3:]
    copies = []
    at = 0
    for i, ref in enumerate(weights):
        rows = ref.shape[0]
        copies.append(pltpu.make_async_copy(ref, out.at[pl.ds(at, rows)], sems.at[i]))
        copies[-1].start()
        at += rows
    for copy in first:
        copy.wait()
    pieces = []
    for ref in gains:
        value = ref[...]
        high = value.astype(bf16).astype(f32)
        rest = value - high
        mid = rest.astype(bf16).astype(f32)
        pieces += [high, mid, rest - mid]
    pieces.append(jnp.zeros((GAIN_ROWS - len(pieces), LANES), f32))
    out[at:, :] = jnp.concatenate(pieces, axis=0).astype(bf16)
    results = tables_of(lengths[...].astype(f32), tokens[...], lax.axis_index("c"))
    for ref, value in zip((table, my_table, spread, entry), results, strict=True):
        ref[...] = value
    for copy in copies:
        copy.wait()


def front(weights, gains, lengths, tokens):
    rows = sum(w.shape[0] for w in weights) + GAIN_ROWS
    slots = tokens.shape[1]
    packed = slots // 2
    shapes = (
        (rows, weights[0].shape[1]),
        (packed, slots),
        (packed // 2, slots),
        (packed, packed),
        (2, tokens.shape[0] // 2, packed),
    )
    small = (*[gain[None, :] for gain in gains], lengths[None, :], tokens)
    count = len(weights) + len(small)
    return pl.pallas_call(
        functools.partial(front_kernel, len(weights)),
        in_specs=[pl.BlockSpec(memory_space=pl.ANY)] * count,
        out_specs=[pl.BlockSpec(memory_space=pltpu.VMEM)] * len(shapes),
        out_shape=[pltpu.VMEM(shape, bf16) for shape in shapes],
        scratch_shapes=[
            pltpu.SemaphoreType.DMA((count,)),
            *[pltpu.VMEM(value.shape, value.dtype) for value in small],
        ],
    )(*weights, *small)


def recur_kernel(sums, lengths, floors, head_gain, states, heads, new_states):
    total = jnp.sum(sums[...].astype(f32), axis=0)
    at = 4 * DK
    stats = total[:, 2 * at :]
    squares = jnp.concatenate(
        [stats[:, 0:1] + stats[:, 1:2], stats[:, 2:3] + stats[:, 3:4]], axis=0
    )
    total = jnp.concatenate([total[:, :at], total[:, at : 2 * at]], axis=0)
    slots = total.shape[0]
    total = total * lax.rsqrt(squares / D + EPSILON)
    queries = total[:, :DK]
    queries = queries * jax.nn.sigmoid(queries)
    fresh = total[:, 2 * DK : 3 * DK]
    gating = total[:, 3 * DK :]
    first = (lax.axis_index("z") * 2 + lax.axis_index("c")) * slots
    slot = iota((slots, 1), 0) + first
    _, own = counted(lengths[...].astype(f32), slot)
    live = ((slot % W).astype(f32) < own).astype(f32)
    floor = floors[...]
    forgets = floor + (1.0 - floor) * jax.nn.sigmoid(total[:, DK : 2 * DK])
    forgets = jnp.where(live > 0, forgets, 1.0)
    both = jnp.concatenate([queries, forgets], axis=0).T
    readings = []
    for seq in range(states.shape[0]):
        carried = states[seq]
        for offset in range(W):
            row = seq * W + offset
            query = both[:, row : row + 1]
            forget = both[:, slots + row : slots + row + 1]
            carried = forget * carried + (1.0 - forget) * fresh[row : row + 1]
            readings.append(jnp.sum(query * carried, axis=0, keepdims=True))
        new_states[seq] = carried
    read_out = jnp.concatenate(readings, axis=0)
    meansq = jnp.mean(read_out * read_out, axis=1, keepdims=True)
    gate = gating * jax.nn.sigmoid(gating)
    out = read_out * lax.rsqrt(meansq + EPSILON) * head_gain[...] * gate * live
    heads[...] = out.astype(bf16)


def recurred(sums, lengths, floors, head_gain, states):
    vmem = pl.BlockSpec(memory_space=pltpu.VMEM)
    return pl.pallas_call(
        recur_kernel,
        in_specs=[vmem] * 5,
        out_specs=[vmem, vmem],
        out_shape=[pltpu.VMEM((2 * sums.shape[1], DK), bf16), pltpu.VMEM(states.shape, f32)],
        compiler_params=SMALL,
    )(*[in_vmem(value) for value in (sums, lengths, floors, head_gain, states)])


def gain_rows(bundle, which):
    at = bundle.shape[0] - GAIN_ROWS + 3 * which
    return jnp.sum(bundle[at : at + 3, :].astype(f32), axis=0, keepdims=True)


def stats_of(own, other, at):
    total = jnp.sum(own * own + other * other, axis=1, keepdims=True)
    upper = total.astype(bf16).astype(f32)
    lanes = iota((1, LANES), 1)
    return jnp.where(lanes == at, upper, jnp.where(lanes == at + 1, total - upper, 0.0))


def products(own, other, gains, weights, product, exact):
    parts = []
    for rows, gain in zip((own, other), gains, strict=True):
        wide = rows * gain
        whole = wide.astype(bf16)
        if exact:
            rest = (wide - whole.astype(f32)).astype(bf16)
            whole = jnp.concatenate([whole, rest], axis=0)
        parts.append(whole)
    count = own.shape[0]
    results = []
    for ours, theirs in weights:
        both = product(parts[0], ours) + product(parts[1], theirs)
        if exact:
            both = both[:count] + both[count:]
        results.append(both)
    return results


def put_rows(sent, results, stats):
    at = 0
    for result in (*results, stats):
        sent[:, at : at + result.shape[1]] = result.astype(bf16)
        at += result.shape[1]


def put_slots(sent, results, stats):
    groups = sent.shape[0]
    width = sum(result.shape[1] for result in results)
    at = 0
    for result in results:
        cols = result.shape[1]
        slots = result.reshape(groups, 2 * W, cols)
        sent[:, :, at : at + cols] = slots[:, :W].astype(bf16)
        sent[:, :, width + at : width + at + cols] = slots[:, W:].astype(bf16)
        at += cols
    low, high = [value.reshape(groups, 2 * W, LANES) for value in stats]
    sent[:, :, 2 * width :] = (low[:, :W] + high[:, W:]).astype(bf16)


def halves_of(weights, bundle, at):
    pairs = []
    for weight in weights:
        pairs.append((weight[...], bundle[at : at + weight.shape[0], :]))
        at += weight.shape[0]
    return pairs


def entry_kernel(gathered, gain, gate, up, bundle, sent, resid):
    cols = gain.shape[1]
    first = lax.axis_index("c") == 0
    groups = gathered.shape[0] // 2
    halves = []
    for at in (0, groups):
        pairs = gathered[at : at + groups].astype(f32)
        rows = pairs.shape[2] // 2
        pairs = jnp.concatenate([pairs[:, :, :rows], pairs[:, :, rows:]], axis=1)
        halves.append(pairs.reshape(cols, rows))
    low, high = halves
    own = jnp.where(first, low, high).T
    other = jnp.where(first, high, low).T
    resid[:, :cols] = own.astype(bf16)
    resid[:, cols:] = other.astype(bf16)
    weights = halves_of((gate, up), bundle, 0)
    gains = (gain[...], gain_rows(bundle, 0))
    results = products(own, other, gains, weights, matmul_t, True)
    put_rows(sent, results, stats_of(own, other, 0))


def mix_kernel(spread, resid, swapped, gain, query, forget, value, outgate, bundle, at, sent):
    cols = gain.shape[1]
    rows = jnp.concatenate([resid[...], swapped[...]], axis=0)
    rows = matmul(spread[...], rows)
    weights = halves_of((query, forget, value, outgate), bundle, at)
    gains = (gain[...], gain_rows(bundle, 1))
    own, other = rows[:, :cols], rows[:, cols:]
    results = products(own, other, gains, weights, matmul, True)
    put_slots(sent, results, (stats_of(own, other, 0), stats_of(own, other, 2)))


def post_kernel(received, before, gain, gate, up, bundle, states, at, sent, resid, out, sem):
    copy = pltpu.make_async_copy(states, out, sem)
    copy.start()
    cols = gain.shape[1]
    total = jnp.sum(received[...].astype(f32), axis=0)
    rows = (before[...].astype(f32) + total).astype(bf16)
    resid[...] = rows
    rows = rows.astype(f32)
    weights = halves_of((gate, up), bundle, at)
    gains = (gain[...], gain_rows(bundle, 2))
    own, other = rows[:, :cols], rows[:, cols:]
    results = products(own, other, gains, weights, matmul_t, False)
    put_rows(sent, results, stats_of(own, other, 0))
    copy.wait()


def post_products(values, states, at, shapes):
    vmem = pl.BlockSpec(memory_space=pltpu.VMEM)
    values = [in_vmem(value) for value in (*values, states)]
    count = len(values)
    return pl.pallas_call(
        lambda *refs: post_kernel(*refs[:count], at, *refs[count:]),
        in_specs=[vmem] * count,
        out_specs=[vmem, vmem, pl.BlockSpec(memory_space=pl.ANY)],
        out_shape=[pltpu.VMEM(shape, bf16) for shape in shapes]
        + [jax.ShapeDtypeStruct(states.shape, f32)],
        scratch_shapes=[pltpu.SemaphoreType.DMA],
        compiler_params=SMALL,
    )(*values)


def put_partials(rows, weight, other, out):
    cols = weight.shape[1]
    own = matmul(rows, weight[...]).astype(bf16)
    other = matmul(rows, other).astype(bf16)
    for i in range(out.shape[0]):
        out[i, :, :cols] = own
        out[i, :, cols:] = other


def hidden_kernel(received, out):
    total = jnp.sum(received[...].astype(f32), axis=0)
    hidden = out.shape[2]
    at = 2 * hidden
    squares = total[:, at : at + 1] + total[:, at + 1 : at + 2]
    scale = lax.rsqrt(squares / D + EPSILON)
    gate = total[:, :hidden] * scale
    up = total[:, hidden:at] * scale
    act = (gate * jax.nn.sigmoid(gate) * up).astype(bf16)
    for i in range(out.shape[0]):
        out[i] = act


def down_kernel(rows, weight, bundle, at, out):
    put_partials(rows[...], weight, bundle[at : at + weight.shape[0], :], out)


def heads_kernel(heads, table, weight, bundle, at, out):
    rows = matmul(table[...], heads[...]).astype(bf16)
    put_partials(rows, weight, bundle[at : at + weight.shape[0], :], out)


def put_pairs(out, at, cols, groups):
    count, rows = cols.shape
    pairs = cols.reshape(groups, count // groups, rows)
    half = count // groups // 2
    paired = jnp.concatenate([pairs[:, :half], pairs[:, half:]], axis=2)
    out[at : at + groups] = paired.astype(out.dtype)


def finish_kernel(rows, resid, weight, bundle, at, out):
    cols = weight.shape[1]
    first = (lax.axis_index("tp") == 0).astype(f32)
    own = 0.5 * matmul(rows[...], weight[...]) + first * resid[:, :cols].astype(f32)
    other = matmul(rows[...], bundle[at : at + weight.shape[0], :])
    other = 0.5 * other + first * resid[:, cols:].astype(f32)
    own, other = own.T, other.T
    leads = lax.axis_index("c") == 0
    groups = out.shape[0] // 2
    put_pairs(out, 0, jnp.where(leads, own, other), groups)
    put_pairs(out, groups, jnp.where(leads, other, own), groups)


def last_kernel(received, table, out):
    groups = received.shape[0] // 2
    half = table.shape[0] // 2
    low = jnp.sum(received[:groups], axis=0)
    high = jnp.sum(received[groups:], axis=0)
    rows = [
        jnp.concatenate([low[:, at : at + half], high[:, at : at + half]], axis=1)
        for at in (0, half)
    ]
    out[...] = matmul(jnp.concatenate(rows, axis=0).astype(bf16), table[...]).astype(bf16)


def last_spread(received, table, cols):
    vmem = pl.BlockSpec(memory_space=pltpu.VMEM)
    return pl.pallas_call(
        last_kernel,
        in_specs=[vmem, vmem],
        out_specs=vmem,
        out_shape=jax.ShapeDtypeStruct((cols, table.shape[1]), bf16),
        compiler_params=SMALL,
    )(in_vmem(received), in_vmem(table))


def in_kernel(kernel, shapes, *values, dtype=bf16):
    vmem = pl.BlockSpec(memory_space=pltpu.VMEM)
    return pl.pallas_call(
        kernel,
        in_specs=[vmem] * len(values),
        out_specs=[vmem] * len(shapes),
        out_shape=[pltpu.VMEM(shape, dtype) for shape in shapes],
        compiler_params=SMALL,
    )(*[in_vmem(value) for value in values])


def local(
    tokens,
    lengths,
    states,
    gain_pre,
    pre_gate,
    pre_up,
    pre_down,
    gain_mix,
    query_weight,
    forget_weight,
    input_weight,
    outgate_weight,
    forget_floor,
    head_gain,
    mix_weight,
    gain_post,
    post_gate,
    post_up,
    post_down,
):
    z_count = lax.axis_size("z")
    tp_count = lax.axis_size("tp")
    slot_count = tokens.shape[0]
    packed = slot_count // 2
    half = packed // 2
    per_z = half // z_count
    own_cols = gain_pre.shape[0]
    hidden = pre_gate.shape[1]
    ff_cols = 2 * hidden
    head_cols = query_weight.shape[1]
    seq_local, heads_local = states.shape[:2]
    swap = [(0, 1), (1, 0)]

    side = {}

    def exchanged(value, axis):
        value, tied = barrier((value, dict(side)))
        value = lax.all_to_all(value, axis, split_axis=0, concat_axis=0, tiled=True)
        value, tied = barrier((value, tied))
        side.update(tied)
        return value

    def sent_to_all(value, axis):
        return exchanged(jnp.broadcast_to(value, (lax.axis_size(axis), *value.shape)), axis)

    mine = (pre_gate.T, pre_up.T, post_gate.T, post_up.T)
    mine += (query_weight, forget_weight, input_weight, outgate_weight)
    mine += (mix_weight, pre_down, post_down)
    gains = (gain_pre, gain_mix, gain_post)
    packed_own, table, my_table, spread, entry = front(mine, gains, lengths, tokens.T)
    bundle = lax.ppermute(packed_own, "c", swap)

    side["table"] = table
    side["my_table"] = my_table
    side["spread"] = spread

    pieces = jnp.broadcast_to(entry[:, None], (2, tp_count, *entry.shape[1:]))
    gathered = exchanged(pieces.reshape(2 * tp_count, *entry.shape[1:]), ("c", "tp"))
    starts = [0]
    for weight in mine:
        starts.append(starts[-1] + weight.shape[0])

    side["bundle"] = bundle
    sent_shape = (half, ff_cols + LANES)
    resid_shape = (half, 2 * own_cols)
    sent, side["resid"] = in_kernel(
        entry_kernel,
        (sent_shape, resid_shape),
        gathered,
        gain_pre[None, :],
        mine[0],
        mine[1],
        bundle,
    )

    def ff_hidden(sent):
        sent = sent.reshape(z_count, per_z, ff_cols + LANES)
        (acts,) = in_kernel(
            hidden_kernel, ((z_count, per_z, hidden),), exchanged(sent, "z")
        )
        return exchanged(acts, "z").reshape(half, hidden)

    partial_shape = (tp_count, *resid_shape)
    act = ff_hidden(sent)
    (partials,) = in_kernel(
        lambda *refs: down_kernel(*refs[:-1], starts[9], refs[-1]),
        (partial_shape,),
        act,
        pre_down,
        side["bundle"],
    )
    summed = jnp.sum(exchanged(partials, "tp").astype(f32), axis=0)
    resid = (side["resid"].astype(f32) + 0.5 * summed).astype(bf16)
    side["resid"] = resid

    turned = jnp.concatenate([resid[:, own_cols:], resid[:, :own_cols]], axis=1)
    swapped = lax.ppermute(turned, "c", swap)
    (sent,) = in_kernel(
        lambda *refs: mix_kernel(*refs[:-1], starts[4], refs[-1]),
        ((z_count, W, 8 * head_cols + LANES),),
        side["spread"],
        resid,
        swapped,
        gain_mix[None, :],
        *mine[4:8],
        side["bundle"],
    )
    side["recur"] = (lengths[None, :], forget_floor[None, :], head_gain[None, :])
    side["states"] = states.reshape(seq_local * heads_local, DK, DK)
    received = exchanged(sent, "z")
    head_out, side["states"] = recurred(received, *side.pop("recur"), side["states"])
    all_heads = sent_to_all(head_out, ("z", "c")).reshape(slot_count, DK)
    (partials,) = in_kernel(
        lambda *refs: heads_kernel(*refs[:-1], starts[8], refs[-1]),
        (partial_shape,),
        all_heads,
        side["my_table"],
        mix_weight,
        side["bundle"],
    )
    received = exchanged(partials, "tp")
    values = (received, side["resid"], gain_post[None, :], mine[2], mine[3], side["bundle"])
    sent, side["resid"], new_states = post_products(
        values, side.pop("states"), starts[2], (sent_shape, resid_shape)
    )
    act = ff_hidden(sent)
    (finish,) = in_kernel(
        lambda *refs: finish_kernel(*refs[:-1], starts[10], refs[-1]),
        ((2 * tp_count, own_cols // tp_count // 2, 2 * half),),
        act,
        side["resid"],
        post_down,
        side["bundle"],
        dtype=f32,
    )
    piece = own_cols // tp_count
    outcome = last_spread(exchanged(finish, ("c", "tp")), side["table"], piece).T
    return (outcome, new_states.reshape(states.shape))


def solution(mesh):
    kv = mesh.shape["kv"]
    tp = mesh.shape["tp"]
    cut = Mesh(mesh.devices.reshape(kv // 2, 2, tp), ("z", "c", "tp"))
    kv_axes = ("z", "c")
    placed = (
        P(None, ("z", "c", "tp")),
        P(),
        P(kv_axes, "tp", None, None),
        P(kv_axes),
        P(kv_axes, "tp"),
        P(kv_axes, "tp"),
        P("tp", kv_axes),
        P(kv_axes),
        P(kv_axes, "tp"),
        P(kv_axes, "tp"),
        P(kv_axes, "tp"),
        P(kv_axes, "tp"),
        P("tp"),
        P(),
        P("tp", kv_axes),
        P(kv_axes),
        P(kv_axes, "tp"),
        P(kv_axes, "tp"),
        P("tp", kv_axes),
    )
    return jax.shard_map(
        local,
        mesh=cut,
        in_specs=placed,
        out_specs=(P(None, ("z", "c", "tp")), P(kv_axes, "tp", None, None)),
        check_vma=False,
    )
```

```python
import functools

import jax
import jax.numpy as jnp
from jax import lax
from jax.experimental import pallas as pl
from jax.experimental.pallas import tpu as pltpu
from jax.sharding import Mesh
from jax.sharding import PartitionSpec as P

D = 4096
DK = 128
W = 4
EPSILON = 1e-06
LANES = 128
GAIN_ROWS = 16

f32 = jnp.float32
bf16 = jnp.bfloat16
barrier = lax.optimization_barrier
SMALL = pltpu.CompilerParams(vmem_limit_bytes=16 * 2**20)


def matmul(a, b):
    return jnp.dot(a, b, preferred_element_type=f32)


def in_vmem(value):
    return pltpu.with_memory_space_constraint(value, pltpu.VMEM)


def matmul_t(a, b):
    return lax.dot_general(a, b, (((1,), (1,)), ((), ())), preferred_element_type=f32)


def iota(shape, axis):
    return lax.broadcasted_iota(jnp.int32, shape, axis)


def tables_of(lengths, tokens, core):
    slots = tokens.shape[1]
    packed = slots // 2
    half = packed // 2
    seqs = lengths.shape[1]
    slot = iota((1, slots), 1)
    seq, seq_of = iota((seqs, slots), 0), iota((seqs, slots), 1) // W
    wide = jnp.broadcast_to(lengths, (8, seqs)).astype(bf16)
    before = matmul(wide, (seq < seq_of).astype(f32).astype(bf16))[:1]
    own = matmul(wide, (seq == seq_of).astype(f32).astype(bf16))[:1]
    within = (slot % W).astype(f32)
    targets = jnp.where(within < own, before + within, -1.0)
    rows = iota((packed, slots), 0).astype(f32)
    table = (rows == targets).astype(f32).astype(bf16)
    rows = (iota((half, slots), 0) + core * half).astype(f32)
    my_table = (rows == targets).astype(f32).astype(bf16)
    place = iota((packed, 1), 0)
    my_slot = place // 8 * 16 + core * 8 + place % 8
    before, own = counted(lengths, my_slot)
    within = (my_slot % W).astype(f32)
    targets = jnp.where(within < own, before + within, -1.0)
    row_ids = ((iota((1, packed), 1) + core * half) % packed).astype(f32)
    spread = (targets == row_ids).astype(f32).astype(bf16)
    entry = matmul_t(tokens, table)
    cols = entry.shape[0] // 2
    entry = jnp.stack(
        [
            jnp.concatenate([entry[:cols, at : at + half], entry[cols:, at : at + half]], axis=1)
            for at in (0, half)
        ]
    ).astype(bf16)
    return table, my_table, spread, entry


def counted(lengths, slots):
    seq = iota((slots.shape[0], lengths.shape[1]), 1)
    before = jnp.sum(jnp.where(seq < slots // W, lengths, 0.0), axis=1, keepdims=True)
    own = jnp.sum(jnp.where(seq == slots // W, lengths, 0.0), axis=1, keepdims=True)
    return before, own


def front_kernel(count, *refs):
    weights, small, refs = refs[:count], refs[count : count + 5], refs[count + 5 :]
    out, table, my_table, spread, entry, sems, *held = refs
    first = []
    for i, (ref, copied) in enumerate(zip(small, held, strict=True)):
        first.append(pltpu.make_async_copy(ref, copied, sems.at[count + i]))
        first[-1].start()
    gains, (lengths, tokens) = held[:3], held[3:]
    copies = []
    at = 0
    for i, ref in enumerate(weights):
        rows = ref.shape[0]
        copies.append(pltpu.make_async_copy(ref, out.at[pl.ds(at, rows)], sems.at[i]))
        copies[-1].start()
        at += rows
    for copy in first:
        copy.wait()
    pieces = []
    for ref in gains:
        value = ref[...]
        high = value.astype(bf16).astype(f32)
        rest = value - high
        mid = rest.astype(bf16).astype(f32)
        pieces += [high, mid, rest - mid]
    pieces.append(jnp.zeros((GAIN_ROWS - len(pieces), LANES), f32))
    out[at:, :] = jnp.concatenate(pieces, axis=0).astype(bf16)
    results = tables_of(lengths[...].astype(f32), tokens[...], lax.axis_index("c"))
    for ref, value in zip((table, my_table, spread, entry), results, strict=True):
        ref[...] = value
    for copy in copies:
        copy.wait()


def front(weights, gains, lengths, tokens):
    rows = sum(w.shape[0] for w in weights) + GAIN_ROWS
    slots = tokens.shape[1]
    packed = slots // 2
    shapes = (
        (rows, weights[0].shape[1]),
        (packed, slots),
        (packed // 2, slots),
        (packed, packed),
        (2, tokens.shape[0] // 2, packed),
    )
    small = (*[gain[None, :] for gain in gains], lengths[None, :], tokens)
    count = len(weights) + len(small)
    return pl.pallas_call(
        functools.partial(front_kernel, len(weights)),
        in_specs=[pl.BlockSpec(memory_space=pl.ANY)] * count,
        out_specs=[pl.BlockSpec(memory_space=pltpu.VMEM)] * len(shapes),
        out_shape=[pltpu.VMEM(shape, bf16) for shape in shapes],
        scratch_shapes=[
            pltpu.SemaphoreType.DMA((count,)),
            *[pltpu.VMEM(value.shape, value.dtype) for value in small],
        ],
    )(*weights, *small)


def recur_kernel(sums, lengths, floors, head_gain, states, heads, new_states):
    total = jnp.sum(sums[...].astype(f32), axis=0)
    at = 4 * DK
    stats = total[:, 2 * at :]
    squares = jnp.concatenate(
        [stats[:, 0:1] + stats[:, 1:2], stats[:, 2:3] + stats[:, 3:4]], axis=0
    )
    total = jnp.concatenate([total[:, :at], total[:, at : 2 * at]], axis=0)
    slots = total.shape[0]
    total = total * lax.rsqrt(squares / D + EPSILON)
    queries = total[:, :DK]
    queries = queries * jax.nn.sigmoid(queries)
    fresh = total[:, 2 * DK : 3 * DK]
    gating = total[:, 3 * DK :]
    first = (lax.axis_index("z") * 2 + lax.axis_index("c")) * slots
    slot = iota((slots, 1), 0) + first
    _, own = counted(lengths[...].astype(f32), slot)
    live = ((slot % W).astype(f32) < own).astype(f32)
    floor = floors[...]
    forgets = floor + (1.0 - floor) * jax.nn.sigmoid(total[:, DK : 2 * DK])
    forgets = jnp.where(live > 0, forgets, 1.0)
    both = jnp.concatenate([queries, forgets], axis=0).T
    readings = []
    for seq in range(states.shape[0]):
        carried = states[seq]
        for offset in range(W):
            row = seq * W + offset
            query = both[:, row : row + 1]
            forget = both[:, slots + row : slots + row + 1]
            carried = forget * carried + (1.0 - forget) * fresh[row : row + 1]
            readings.append(jnp.sum(query * carried, axis=0, keepdims=True))
        new_states[seq] = carried
    read_out = jnp.concatenate(readings, axis=0)
    meansq = jnp.mean(read_out * read_out, axis=1, keepdims=True)
    gate = gating * jax.nn.sigmoid(gating)
    out = read_out * lax.rsqrt(meansq + EPSILON) * head_gain[...] * gate * live
    heads[...] = out.astype(bf16)


def recurred(sums, lengths, floors, head_gain, states):
    vmem = pl.BlockSpec(memory_space=pltpu.VMEM)
    return pl.pallas_call(
        recur_kernel,
        in_specs=[vmem] * 5,
        out_specs=[vmem, vmem],
        out_shape=[pltpu.VMEM((2 * sums.shape[1], DK), bf16), pltpu.VMEM(states.shape, f32)],
        compiler_params=SMALL,
    )(*[in_vmem(value) for value in (sums, lengths, floors, head_gain, states)])


def gain_rows(bundle, which):
    at = bundle.shape[0] - GAIN_ROWS + 3 * which
    return jnp.sum(bundle[at : at + 3, :].astype(f32), axis=0, keepdims=True)


def stats_of(own, other, at):
    total = jnp.sum(own * own + other * other, axis=1, keepdims=True)
    upper = total.astype(bf16).astype(f32)
    lanes = iota((1, LANES), 1)
    return jnp.where(lanes == at, upper, jnp.where(lanes == at + 1, total - upper, 0.0))


def products(own, other, gains, weights, product, exact):
    parts = []
    for rows, gain in zip((own, other), gains, strict=True):
        wide = rows * gain
        whole = wide.astype(bf16)
        if exact:
            rest = (wide - whole.astype(f32)).astype(bf16)
            whole = jnp.concatenate([whole, rest], axis=0)
        parts.append(whole)
    count = own.shape[0]
    results = []
    for ours, theirs in weights:
        both = product(parts[0], ours) + product(parts[1], theirs)
        if exact:
            both = both[:count] + both[count:]
        results.append(both)
    return results


def put_rows(sent, results, stats):
    at = 0
    for result in (*results, stats):
        sent[:, at : at + result.shape[1]] = result.astype(bf16)
        at += result.shape[1]


def put_slots(sent, results, stats):
    groups = sent.shape[0]
    width = sum(result.shape[1] for result in results)
    at = 0
    for result in results:
        cols = result.shape[1]
        slots = result.reshape(groups, 2 * W, cols)
        sent[:, :, at : at + cols] = slots[:, :W].astype(bf16)
        sent[:, :, width + at : width + at + cols] = slots[:, W:].astype(bf16)
        at += cols
    low, high = [value.reshape(groups, 2 * W, LANES) for value in stats]
    sent[:, :, 2 * width :] = (low[:, :W] + high[:, W:]).astype(bf16)


def halves_of(weights, bundle, at):
    pairs = []
    for weight in weights:
        pairs.append((weight[...], bundle[at : at + weight.shape[0], :]))
        at += weight.shape[0]
    return pairs


def entry_kernel(gathered, gain, gate, up, bundle, sent, resid):
    cols = gain.shape[1]
    first = lax.axis_index("c") == 0
    groups = gathered.shape[0] // 2
    halves = []
    for at in (0, groups):
        pairs = gathered[at : at + groups].astype(f32)
        rows = pairs.shape[2] // 2
        pairs = jnp.concatenate([pairs[:, :, :rows], pairs[:, :, rows:]], axis=1)
        halves.append(pairs.reshape(cols, rows))
    low, high = halves
    own = jnp.where(first, low, high).T
    other = jnp.where(first, high, low).T
    resid[:, :cols] = own.astype(bf16)
    resid[:, cols:] = other.astype(bf16)
    weights = halves_of((gate, up), bundle, 0)
    gains = (gain[...], gain_rows(bundle, 0))
    results = products(own, other, gains, weights, matmul_t, True)
    put_rows(sent, results, stats_of(own, other, 0))


def mix_rows(rows, gain, weights, bundle, at):
    cols = gain.shape[1]
    rows = rows[...].astype(f32)
    own, other = rows[:, :cols], rows[:, cols:]
    gains = (gain[...], gain_rows(bundle, 1))
    results = products(own, other, gains, halves_of(weights, bundle, at), matmul, True)
    stats = [stats_of(own, other, 0), stats_of(own, other, 2)]
    return jnp.concatenate([value.astype(bf16) for value in (*results, *stats)], axis=1)


def own_kernel(rows, gain, query, forget, value, outgate, bundle, at, out):
    out[...] = mix_rows(rows, gain, (query, forget, value, outgate), bundle, at)


def mix_kernel(spread, ready, rows, gain, query, forget, value, outgate, bundle, at, sent):
    others = mix_rows(rows, gain, (query, forget, value, outgate), bundle, at)
    slots = matmul(spread[...], jnp.concatenate([ready[...], others], axis=0))
    width = slots.shape[1] - 2 * LANES
    stats = (slots[:, width : width + LANES], slots[:, width + LANES :])
    put_slots(sent, [slots[:, :width]], stats)


def post_kernel(received, before, gain, gate, up, bundle, states, at, sent, resid, out, sem):
    copy = pltpu.make_async_copy(states, out, sem)
    copy.start()
    cols = gain.shape[1]
    total = jnp.sum(received[...].astype(f32), axis=0)
    rows = (before[...].astype(f32) + total).astype(bf16)
    resid[...] = rows
    rows = rows.astype(f32)
    weights = halves_of((gate, up), bundle, at)
    gains = (gain[...], gain_rows(bundle, 2))
    own, other = rows[:, :cols], rows[:, cols:]
    results = products(own, other, gains, weights, matmul_t, False)
    put_rows(sent, results, stats_of(own, other, 0))
    copy.wait()


def post_products(values, states, at, shapes):
    vmem = pl.BlockSpec(memory_space=pltpu.VMEM)
    values = [in_vmem(value) for value in (*values, states)]
    count = len(values)
    return pl.pallas_call(
        lambda *refs: post_kernel(*refs[:count], at, *refs[count:]),
        in_specs=[vmem] * count,
        out_specs=[vmem, vmem, pl.BlockSpec(memory_space=pl.ANY)],
        out_shape=[pltpu.VMEM(shape, bf16) for shape in shapes]
        + [jax.ShapeDtypeStruct(states.shape, f32)],
        scratch_shapes=[pltpu.SemaphoreType.DMA],
        compiler_params=SMALL,
    )(*values)


def put_partials(rows, weight, other, out):
    cols = weight.shape[1]
    own = matmul(rows, weight[...]).astype(bf16)
    other = matmul(rows, other).astype(bf16)
    for i in range(out.shape[0]):
        out[i, :, :cols] = own
        out[i, :, cols:] = other


def hidden_kernel(received, out):
    total = jnp.sum(received[...].astype(f32), axis=0)
    hidden = out.shape[2]
    at = 2 * hidden
    squares = total[:, at : at + 1] + total[:, at + 1 : at + 2]
    scale = lax.rsqrt(squares / D + EPSILON)
    gate = total[:, :hidden] * scale
    up = total[:, hidden:at] * scale
    act = (gate * jax.nn.sigmoid(gate) * up).astype(bf16)
    for i in range(out.shape[0]):
        out[i] = act


def down_kernel(rows, weight, bundle, at, out):
    put_partials(rows[...], weight, bundle[at : at + weight.shape[0], :], out)


def heads_kernel(heads, table, weight, bundle, at, out):
    rows = matmul(table[...], heads[...]).astype(bf16)
    put_partials(rows, weight, bundle[at : at + weight.shape[0], :], out)


def put_pairs(out, at, cols, groups):
    count, rows = cols.shape
    pairs = cols.reshape(groups, count // groups, rows)
    half = count // groups // 2
    paired = jnp.concatenate([pairs[:, :half], pairs[:, half:]], axis=2)
    out[at : at + groups] = paired.astype(out.dtype)


def finish_kernel(rows, resid, weight, bundle, at, out):
    cols = weight.shape[1]
    first = (lax.axis_index("tp") == 0).astype(f32)
    own = 0.5 * matmul(rows[...], weight[...]) + first * resid[:, :cols].astype(f32)
    other = matmul(rows[...], bundle[at : at + weight.shape[0], :])
    other = 0.5 * other + first * resid[:, cols:].astype(f32)
    own, other = own.T, other.T
    leads = lax.axis_index("c") == 0
    groups = out.shape[0] // 2
    put_pairs(out, 0, jnp.where(leads, own, other), groups)
    put_pairs(out, groups, jnp.where(leads, other, own), groups)


def last_kernel(received, table, out):
    groups = received.shape[0] // 2
    half = table.shape[0] // 2
    low = jnp.sum(received[:groups], axis=0)
    high = jnp.sum(received[groups:], axis=0)
    rows = [
        jnp.concatenate([low[:, at : at + half], high[:, at : at + half]], axis=1)
        for at in (0, half)
    ]
    out[...] = matmul(jnp.concatenate(rows, axis=0).astype(bf16), table[...]).astype(bf16)


def last_spread(received, table, cols):
    vmem = pl.BlockSpec(memory_space=pltpu.VMEM)
    return pl.pallas_call(
        last_kernel,
        in_specs=[vmem, vmem],
        out_specs=vmem,
        out_shape=jax.ShapeDtypeStruct((cols, table.shape[1]), bf16),
        compiler_params=SMALL,
    )(in_vmem(received), in_vmem(table))


def in_kernel(kernel, shapes, *values, dtype=bf16):
    vmem = pl.BlockSpec(memory_space=pltpu.VMEM)
    return pl.pallas_call(
        kernel,
        in_specs=[vmem] * len(values),
        out_specs=[vmem] * len(shapes),
        out_shape=[pltpu.VMEM(shape, dtype) for shape in shapes],
        compiler_params=SMALL,
    )(*[in_vmem(value) for value in values])


def local(
    tokens,
    lengths,
    states,
    gain_pre,
    pre_gate,
    pre_up,
    pre_down,
    gain_mix,
    query_weight,
    forget_weight,
    input_weight,
    outgate_weight,
    forget_floor,
    head_gain,
    mix_weight,
    gain_post,
    post_gate,
    post_up,
    post_down,
):
    z_count = lax.axis_size("z")
    tp_count = lax.axis_size("tp")
    slot_count = tokens.shape[0]
    packed = slot_count // 2
    half = packed // 2
    per_z = half // z_count
    own_cols = gain_pre.shape[0]
    hidden = pre_gate.shape[1]
    ff_cols = 2 * hidden
    head_cols = query_weight.shape[1]
    seq_local, heads_local = states.shape[:2]
    swap = [(0, 1), (1, 0)]

    side = {}

    def exchanged(value, axis):
        value, tied = barrier((value, dict(side)))
        value = lax.all_to_all(value, axis, split_axis=0, concat_axis=0, tiled=True)
        value, tied = barrier((value, tied))
        side.update(tied)
        return value

    def sent_to_all(value, axis):
        return exchanged(jnp.broadcast_to(value, (lax.axis_size(axis), *value.shape)), axis)

    mine = (pre_gate.T, pre_up.T, post_gate.T, post_up.T)
    mine += (query_weight, forget_weight, input_weight, outgate_weight)
    mine += (mix_weight, pre_down, post_down)
    gains = (gain_pre, gain_mix, gain_post)
    packed_own, table, my_table, spread, entry = front(mine, gains, lengths, tokens.T)
    bundle = lax.ppermute(packed_own, "c", swap)

    side["table"] = table
    side["my_table"] = my_table
    side["spread"] = spread

    pieces = jnp.broadcast_to(entry[:, None], (2, tp_count, *entry.shape[1:]))
    gathered = exchanged(pieces.reshape(2 * tp_count, *entry.shape[1:]), ("c", "tp"))
    starts = [0]
    for weight in mine:
        starts.append(starts[-1] + weight.shape[0])

    side["bundle"] = bundle
    sent_shape = (half, ff_cols + LANES)
    resid_shape = (half, 2 * own_cols)
    sent, side["resid"] = in_kernel(
        entry_kernel,
        (sent_shape, resid_shape),
        gathered,
        gain_pre[None, :],
        mine[0],
        mine[1],
        bundle,
    )

    def ff_hidden(sent):
        sent = sent.reshape(z_count, per_z, ff_cols + LANES)
        (acts,) = in_kernel(
            hidden_kernel, ((z_count, per_z, hidden),), exchanged(sent, "z")
        )
        return exchanged(acts, "z").reshape(half, hidden)

    partial_shape = (tp_count, *resid_shape)
    act = ff_hidden(sent)
    (partials,) = in_kernel(
        lambda *refs: down_kernel(*refs[:-1], starts[9], refs[-1]),
        (partial_shape,),
        act,
        pre_down,
        side["bundle"],
    )
    summed = jnp.sum(exchanged(partials, "tp").astype(f32), axis=0)
    resid = (side["resid"].astype(f32) + 0.5 * summed).astype(bf16)
    side["resid"] = resid

    turned = jnp.concatenate([resid[:, own_cols:], resid[:, :own_cols]], axis=1)
    swapped = lax.ppermute(turned, "c", swap)
    mix_values = (gain_mix[None, :], *mine[4:8], side["bundle"])
    (ready,) = in_kernel(
        lambda *refs: own_kernel(*refs[:-1], starts[4], refs[-1]),
        ((half, 4 * head_cols + 2 * LANES),),
        resid,
        *mix_values,
    )
    (sent,) = in_kernel(
        lambda *refs: mix_kernel(*refs[:-1], starts[4], refs[-1]),
        ((z_count, W, 8 * head_cols + LANES),),
        side["spread"],
        ready,
        swapped,
        *mix_values,
    )
    side["recur"] = (lengths[None, :], forget_floor[None, :], head_gain[None, :])
    side["states"] = states.reshape(seq_local * heads_local, DK, DK)
    received = exchanged(sent, "z")
    head_out, side["states"] = recurred(received, *side.pop("recur"), side["states"])
    all_heads = sent_to_all(head_out, ("z", "c")).reshape(slot_count, DK)
    (partials,) = in_kernel(
        lambda *refs: heads_kernel(*refs[:-1], starts[8], refs[-1]),
        (partial_shape,),
        all_heads,
        side["my_table"],
        mix_weight,
        side["bundle"],
    )
    received = exchanged(partials, "tp")
    values = (received, side["resid"], gain_post[None, :], mine[2], mine[3], side["bundle"])
    sent, side["resid"], new_states = post_products(
        values, side.pop("states"), starts[2], (sent_shape, resid_shape)
    )
    act = ff_hidden(sent)
    (finish,) = in_kernel(
        lambda *refs: finish_kernel(*refs[:-1], starts[10], refs[-1]),
        ((2 * tp_count, own_cols // tp_count // 2, 2 * half),),
        act,
        side["resid"],
        post_down,
        side["bundle"],
        dtype=f32,
    )
    piece = own_cols // tp_count
    outcome = last_spread(exchanged(finish, ("c", "tp")), side["table"], piece).T
    return (outcome, new_states.reshape(states.shape))


def solution(mesh):
    kv = mesh.shape["kv"]
    tp = mesh.shape["tp"]
    cut = Mesh(mesh.devices.reshape(kv // 2, 2, tp), ("z", "c", "tp"))
    kv_axes = ("z", "c")
    placed = (
        P(None, ("z", "c", "tp")),
        P(),
        P(kv_axes, "tp", None, None),
        P(kv_axes),
        P(kv_axes, "tp"),
        P(kv_axes, "tp"),
        P("tp", kv_axes),
        P(kv_axes),
        P(kv_axes, "tp"),
        P(kv_axes, "tp"),
        P(kv_axes, "tp"),
        P(kv_axes, "tp"),
        P("tp"),
        P(),
        P("tp", kv_axes),
        P(kv_axes),
        P(kv_axes, "tp"),
        P(kv_axes, "tp"),
        P("tp", kv_axes),
    )
    return jax.shard_map(
        local,
        mesh=cut,
        in_specs=placed,
        out_specs=(P(None, ("z", "c", "tp")), P(kv_axes, "tp", None, None)),
        check_vma=False,
    )
```
